32 devices in a mesh: sp: 16 (over z, y, x), tp: 2 (over core).
Axes of the slice: x: 2, y: 2, z: 4, core: 2. Of those that a mesh axis runs over, the one named last changes fastest.
Arguments:
- residual: bfloat16 [4096, 2048], P(('sp', 'tp')), may hold values from -6 to 6
- query_nope: bfloat16 [4096, 1024], P('sp', 'tp'), may hold values from -24 to 24
- query_rope: bfloat16 [4096, 512], P('sp', 'tp'), may hold values from -400 to 400
- latent: bfloat16 [4096, 256], P(('sp', 'tp')), may hold values from -6 to 6
- key_rope: bfloat16 [4096, 64], P(('sp', 'tp')), may hold values from -6 to 6
- key_up: bfloat16 [256, 1024], P(None, 'tp'), may hold values from -0.375 to 0.375
- value_up: bfloat16 [256, 1024], P(None, 'tp'), may hold values from -0.375 to 0.375
- out_proj: bfloat16 [1024, 2048], replicated, may hold values from -0.375 to 0.375
- norm_gain: float32 [2048], replicated, may hold values from 0.1 to 1.9
- routes: int32 [4096, 2], P(('sp', 'tp')), may hold values from 0 to 15, all different within a row; in each aligned block of 128 rows (0 to 127, 128 to 255, ...) at most 32 rows name the same one
- route_weight: float32 [4096, 2], P(('sp', 'tp')), may hold values from 0.3 to 2.5
- w_gate: bfloat16 [16, 2048, 512], P('sp', None, 'tp'), may hold values from -0.125 to 0.125
- w_up: bfloat16 [16, 2048, 512], P('sp', None, 'tp'), may hold values from -0.125 to 0.125
- w_down: bfloat16 [16, 512, 2048], P('sp', 'tp'), may hold values from -0.25 to 0.25
Outputs:
- mixed: bfloat16 [4096, 2048], P(('sp', 'tp'))
The draws below stay inside these ranges and needn't reach their ends.
Inputs may be any that keep to these rules, and one draw needn't show every extreme that they name: `routes`: each row names 2 different experts. Among the rows of one device no expert is named more than 32 times, a bound that some block reaches by the rows of some device.
All inputs are finite; a program needn't handle non-finite values.
Results may differ from the reference program's by a relative error of at most 0.015.
Values may be sent and summed in bfloat16 or wider, within the bound.
A program may use at most 128 MiB of HBM per device.

```python
import math
import jax
import jax.numpy as jnp
import numpy as np
from jax import lax

D = 2048
HEADS = 8
QK_NOPE = 128
QK_ROPE = 64
V_DIM = 128
LATENT = 256
FF = 512
TOP = 2
SEGMENT = 64
TOK_DEV = 256
TOKENS = 4096
EXPERTS = 16
CAP = 32
N_SP = 16
N_TP = 2


def draw_key_rope(key, part):
    noise = jax.random.truncated_normal(jax.random.fold_in(key, 31), -6.0, 6.0, (TOKENS, QK_ROPE), jnp.float32)
    return noise.astype(jnp.bfloat16)


def draw_query_rope(key, part):
    noise = jax.random.truncated_normal(jax.random.fold_in(key, 32), -6.0, 6.0, (TOKENS, HEADS * QK_ROPE), jnp.float32)
    return noise.astype(jnp.bfloat16)


def steps_of(rng, dims, shards, low, largest):
    loudness, own = 1.0, jax.random.fold_in(rng, 6)
    for dim, blocks in shards:
        heights = jnp.exp(jax.random.uniform(jax.random.fold_in(own, dim), (blocks,), jnp.float32, low / len(shards), largest / len(shards)))
        loudness = loudness * jnp.repeat(heights, dims[dim] // blocks).reshape([-1 if axis == dim else 1 for axis in range(len(dims))])
    return loudness


def routed_block(key, own, number, rows, number_of, top, reach, skew):
    order = jax.random.permutation(key, number_of)
    crowded, usual = load_shares(number_of, rows * top, reach, skew, True), load_shares(number_of, rows * top, reach, skew, False)
    places = jnp.arange(number_of)

    def named(sizes, turn):
        used = int((sizes > 0).sum())
        fixed = max(1, used // 4)
        moved = fixed + (places - fixed + turn * (used - fixed)) % max(1, number_of - fixed)
        return jnp.zeros((number_of,), jnp.int32).at[order[jnp.where(places < fixed, places, moved)]].set(jnp.asarray(sizes, jnp.int32))

    sizes = jnp.where(number % 4 == 0, named(crowded, number // 4), named(usual, number - number // 4 - 1))
    mixed = jax.random.permutation(jax.random.fold_in(own, 3), number_of)
    donor, taker = mixed[0:number_of // 2 * 2:2], mixed[1:number_of // 2 * 2:2]
    slack = jnp.minimum(sizes[donor] - 1, reach - sizes[taker]) // 2
    slack = jnp.where((donor == order[0]) | (taker == order[0]) | (sizes[taker] == 0), 0, jnp.maximum(slack, 0))
    moved = jax.random.randint(jax.random.fold_in(own, 4), (number_of // 2,), 0, 1 << 20) % (slack + 1)
    sizes = sizes.at[donor].add(-moved).at[taker].add(moved)
    items = jnp.searchsorted(jnp.cumsum(sizes), jnp.arange(rows * top), side="right").astype(jnp.int32)
    grid = items.reshape(top, rows).T
    grid = grid[jax.random.permutation(jax.random.fold_in(own, 1), rows)]
    turn = jax.random.randint(jax.random.fold_in(own, 2), (rows, 1), 0, top)
    return jnp.take_along_axis(grid, (jnp.arange(top)[None, :] + turn) % top, axis=1)


def load_shares(count, total, most, slope, full):
    weights = [(1 << 20) // math.isqrt(standing ** slope) + 1 for standing in range(1, count + 1)]
    largest = most if full else min(most, max(-(-total // count), total * weights[0] // sum(weights)))
    least = 1 if total - largest >= count - 1 else 0
    holding, surplus = [largest] + [least] * (count - 1), total - largest - least * (count - 1)
    while surplus > 0:
        movable = [i for i in range(1, count) if holding[i] < largest] or [i for i in range(1, count) if holding[i] < most]
        whole, budget = sum([weights[i] for i in movable]), surplus
        for i in movable:
            addition = min(most - holding[i], max(1, budget * weights[i] // whole), surplus)
            holding[i] = holding[i] + addition
            surplus = surplus - addition
    return np.array(holding)


def normal_values(own_key, shape, width, most, split=(), held_as=jnp.bfloat16):
    values = jax.random.normal(own_key, shape, jnp.float32) * width
    if len(split) > 0:
        values = steps_of(own_key, shape, split, -0.22, 0.18) * values
    return jnp.clip(values, min=-most, max=most).astype(held_as)


def setup_inputs(seed: int = 0) -> dict:
    keys = jax.random.split(jax.random.key(seed), 15)
    residual = normal_values(keys[0], (TOKENS, D), 1.0, 6.0, ((0, 32),))
    query_nope = normal_values(keys[1], (TOKENS, HEADS * QK_NOPE), 4.0, 24.0, ((0, 16), (1, 2)))
    query_rope = draw_query_rope(jax.random.fold_in(keys[14], 71), 0)
    latent = normal_values(keys[3], (TOKENS, LATENT), 1.0, 6.0, ((0, 32),))
    key_rope = draw_key_rope(jax.random.fold_in(keys[14], 71), 0)
    key_up = normal_values(keys[5], (LATENT, HEADS * QK_NOPE), LATENT ** -0.5, 0.375, ((1, 2),))
    value_up = normal_values(keys[6], (LATENT, HEADS * V_DIM), LATENT ** -0.5, 0.375, ((1, 2),))
    out_proj = normal_values(keys[7], (HEADS * V_DIM, D), (HEADS * V_DIM // 4) ** -0.5, 0.375)
    norm_gain = jnp.clip(1.0 + 0.18 * jax.random.normal(keys[8], (D,), jnp.float32), 0.1, 1.9)
    routes_keys = jax.random.split(jax.random.fold_in(keys[9], 1), TOKENS // (TOK_DEV // N_TP))
    routes_turns = jax.random.permutation(jax.random.fold_in(keys[9], 3), TOKENS // (TOK_DEV // N_TP))
    routes = jax.vmap(lambda own, number: routed_block(jax.random.fold_in(keys[9], 2), own, number, TOK_DEV // N_TP, EXPERTS, TOP, CAP, 2))(routes_keys, routes_turns).reshape((TOKENS, TOP))
    route_weight = jnp.clip(jnp.exp(math.log(2.5) - 2.1202635 * jax.random.uniform(keys[10], (TOKENS, TOP), jnp.float32) ** steps_of(keys[10], (TOKENS, TOP), ((0, 32),), -0.2, 0.2)), 0.3, 2.5)
    w_gate = normal_values(keys[11], (EXPERTS, D, FF), D ** -0.5, 0.125, ((0, 16), (2, 2)))
    w_up = normal_values(keys[12], (EXPERTS, D, FF), D ** -0.5, 0.125, ((0, 16), (2, 2)))
    w_down = normal_values(keys[13], (EXPERTS, FF, D), FF ** -0.5, 0.25, ((0, 16), (1, 2)))
    return dict(residual=residual, query_nope=query_nope, query_rope=query_rope, latent=latent, key_rope=key_rope, key_up=key_up, value_up=value_up, out_proj=out_proj, norm_gain=norm_gain, routes=routes, route_weight=route_weight, w_gate=w_gate, w_up=w_up, w_down=w_down)


EPSILON = 1e-06
ROPE_BASE = 10000.0

def rotary(values, positions):
    half_width = values.shape[-1] // 2
    inverse = ROPE_BASE ** (-2.0 * jnp.arange(half_width, dtype=jnp.float32) / values.shape[-1])
    angles = positions.astype(jnp.float32)[:, None] * inverse[None, :]
    cosine = jnp.cos(angles)
    sine_part = jnp.sin(angles)
    if values.ndim == 3:
        cosine = cosine[:, None, :]
        sine_part = sine_part[:, None, :]
    first_half = values[..., :half_width]
    second = values[..., half_width:]
    return jnp.concatenate([first_half * cosine - second * sine_part, second * cosine + first_half * sine_part], axis=-1)

def reference(residual, query_nope, query_rope, latent, key_rope, key_up, value_up, out_proj, norm_gain, routes, route_weight, w_gate, w_up, w_down):
    positions = jnp.arange(TOKENS, dtype=jnp.int32)
    query_rot = rotary(query_rope.astype(jnp.float32).reshape(TOKENS, HEADS, QK_ROPE), positions).astype(jnp.bfloat16)
    key_rot = rotary(key_rope.astype(jnp.float32), positions).astype(jnp.bfloat16)
    key_nope = jnp.dot(latent, key_up, preferred_element_type=jnp.float32).astype(jnp.bfloat16)
    value_rows = jnp.dot(latent, value_up, preferred_element_type=jnp.float32).astype(jnp.bfloat16)
    keys_wide = key_nope.astype(jnp.float32).reshape(TOKENS, HEADS, QK_NOPE)
    values_wide = value_rows.astype(jnp.float32).reshape(TOKENS, HEADS, V_DIM)
    rot_wide = key_rot.astype(jnp.float32)
    query_wide = query_nope.astype(jnp.float32).reshape(TOKENS, HEADS, QK_NOPE)
    query_rot_wide = query_rot.astype(jnp.float32)
    score_scale = (QK_NOPE + QK_ROPE) ** (-0.5)
    key_segment = positions // SEGMENT
    query_block = math.gcd(TOKENS, 512)

    def one_block(block_index):
        first_row = (block_index * query_block).astype(jnp.int32)
        query_part = lax.dynamic_slice_in_dim(query_wide, first_row, query_block, 0)
        rot_part = lax.dynamic_slice_in_dim(query_rot_wide, first_row, query_block, 0)
        scores = jnp.einsum('qhd,khd->hqk', query_part, keys_wide)
        scores = (scores + jnp.einsum('qhr,kr->hqk', rot_part, rot_wide)) * score_scale
        query_segment = (first_row + jnp.arange(query_block, dtype=jnp.int32)) // SEGMENT
        allowed = (key_segment[None, :] <= query_segment[:, None])[None]
        scores = jnp.where(allowed, scores, -jnp.inf)
        row_max = lax.optimization_barrier(jnp.max(scores, axis=-1, keepdims=True))
        weights = jnp.exp(scores - row_max)
        weight_sum = lax.optimization_barrier(jnp.sum(weights, axis=-1))
        weights_low = lax.optimization_barrier(weights.astype(jnp.bfloat16)).astype(jnp.float32)
        weighted = jnp.einsum('hqk,khv->qhv', weights_low, values_wide)
        return weighted / weight_sum.T[:, :, None]
    attn_out = lax.map(one_block, jnp.arange(TOKENS // query_block, dtype=jnp.int32))
    attn_out = attn_out.reshape(TOKENS, HEADS * V_DIM).astype(jnp.bfloat16)
    projected = jnp.dot(attn_out, out_proj, preferred_element_type=jnp.float32)
    hidden = (residual.astype(jnp.float32) + projected).astype(jnp.bfloat16)
    hidden_wide = hidden.astype(jnp.float32)
    normed = hidden_wide * lax.rsqrt(lax.optimization_barrier(jnp.mean(hidden_wide * hidden_wide, axis=-1, keepdims=True)) + EPSILON)
    normed = (normed * norm_gain[None, :]).astype(jnp.bfloat16)
    buffer_rows = N_TP * N_SP * CAP
    flat_expert = routes.reshape(-1).astype(jnp.int32)
    onehot = (flat_expert[:, None] == jnp.arange(EXPERTS, dtype=jnp.int32)[None, :]).astype(jnp.int32)
    slot_rank = lax.optimization_barrier(jnp.sum(jnp.cumsum(onehot, axis=0) * onehot, axis=1)) - 1
    slot_index = (flat_expert * buffer_rows + slot_rank).astype(jnp.int32)
    buffer = jnp.zeros((EXPERTS * buffer_rows, D), jnp.bfloat16).at[slot_index].set(jnp.repeat(normed, TOP, axis=0))

    def expert_rows(inputs):
        rows_in, gate_weight, up_weight, down_weight = inputs
        gate_part = jnp.dot(rows_in, gate_weight, preferred_element_type=jnp.float32)
        up_part = jnp.dot(rows_in, up_weight, preferred_element_type=jnp.float32)
        activated = lax.optimization_barrier((jax.nn.silu(gate_part) * up_part).astype(jnp.bfloat16))
        parts = jnp.einsum('bpf,pfd->pbd', activated.astype(jnp.float32).reshape(buffer_rows, N_TP, FF // N_TP), down_weight.astype(jnp.float32).reshape(N_TP, FF // N_TP, D))
        half_out = lax.optimization_barrier(parts.astype(jnp.bfloat16)).astype(jnp.float32)
        return lax.optimization_barrier(jnp.sum(half_out, axis=0)).astype(jnp.bfloat16)
    outputs = lax.map(expert_rows, (buffer.reshape(EXPERTS, buffer_rows, D), w_gate, w_up, w_down))
    picked = outputs.reshape(EXPERTS * buffer_rows, D)[slot_index]
    combined = lax.optimization_barrier(jnp.sum(picked.astype(jnp.float32).reshape(TOKENS, TOP, D) * route_weight[:, :, None], axis=1))
    return (hidden_wide + combined).astype(jnp.bfloat16)
```

```python
import functools
import math

import jax
import jax.numpy as jnp
from jax import lax
from jax.experimental import pallas as pl
from jax.experimental.pallas import tpu as pltpu
from jax.sharding import PartitionSpec as P

QK_NOPE = 128
QK_ROPE = 64
V_DIM = 128
SEGMENT = 64


EPSILON = 1e-06
ROPE_BASE = 10000.0
NEG_LARGE = -1e30


def rotary(values, positions):
    half_width = values.shape[-1] // 2
    inverse = ROPE_BASE ** (-2.0 * jnp.arange(half_width, dtype=jnp.float32) / values.shape[-1])
    angles = positions.astype(jnp.float32)[:, None] * inverse[None, :]
    cosine = jnp.cos(angles)
    sine_part = jnp.sin(angles)
    if values.ndim == 3:
        cosine = cosine[:, None, :]
        sine_part = sine_part[:, None, :]
    first_half = values[..., :half_width]
    second = values[..., half_width:]
    return jnp.concatenate(
        [first_half * cosine - second * sine_part, second * cosine + first_half * sine_part],
        axis=-1,
    )


MESH = pl.DeviceIdType.MESH
VMEM = pl.BlockSpec(memory_space=pltpu.VMEM)


def greet(peers):
    barrier = pltpu.get_barrier_semaphore()
    for peer in peers:
        pl.semaphore_signal(barrier, inc=1, device_id=peer, device_id_type=MESH)
    pl.semaphore_wait(barrier, len(peers))


def far_first(count):
    return sorted(range(1, count), key=lambda step: abs(2 * step - count))


def send(source, target, send_sem, recv_sem, peer):
    copy = pltpu.make_async_remote_copy(
        src_ref=source,
        dst_ref=target,
        send_sem=send_sem,
        recv_sem=recv_sem,
        device_id=peer,
        device_id_type=MESH,
    )
    copy.start()
    return copy


def arrived(block, semaphore):
    pltpu.make_async_copy(block, block, semaphore).wait()


def gather_kernel(n_sp, n_tp, inner, own_ref, out_ref, send_sem, recv_sem, local_sem):
    sp, tp = lax.axis_index("sp"), lax.axis_index("tp")
    outer = n_sp // inner
    group, member = sp // inner, sp % inner

    def column(step):
        return ((group + step) % outer) * inner + member

    def mate(step):
        return group * inner + (member + step) % inner

    others = [(column(step), tp) for step in far_first(outer)]
    mates = [(mate(step), tp) for step in range(1, inner)]
    twins = [(sp, (tp + step) % n_tp) for step in range(1, n_tp)]
    greet(others + mates + twins)
    copies = []

    def push(source, block, peers):
        for peer in peers:
            copies.append(
                send(
                    source, out_ref.at[block], send_sem.at[len(copies)], recv_sem.at[block], peer
                )
            )

    mine = sp * n_tp + tp
    keep = pltpu.make_async_copy(own_ref, out_ref.at[mine], local_sem)
    keep.start()
    push(own_ref, mine, others + mates + twins)
    for step in sorted(range(1, outer), key=lambda step: min(step, outer - step)):
        block = column(step) * n_tp + tp
        arrived(out_ref.at[block], recv_sem.at[block])
        push(out_ref.at[block], block, mates + twins)
    for step in range(outer):
        for hop in range(1, inner):
            source = ((group + step) % outer) * inner + (member + hop) % inner
            block = source * n_tp + tp
            arrived(out_ref.at[block], recv_sem.at[block])
            push(out_ref.at[block], block, twins)
    for twin in twins:
        for source in range(n_sp):
            block = source * n_tp + twin[1]
            arrived(out_ref.at[block], recv_sem.at[block])
    keep.wait()
    for copy in copies:
        copy.wait_send()


def gather_rows(own, n_sp, n_tp):
    inner = math.gcd(n_sp, 4)
    outer = n_sp // inner
    sends = (outer - 1) + outer * (inner - 1) + n_sp * (n_tp - 1)
    return pl.pallas_call(
        functools.partial(gather_kernel, n_sp, n_tp, inner),
        out_shape=jax.ShapeDtypeStruct((n_sp * n_tp,) + own.shape, own.dtype),
        in_specs=[VMEM],
        out_specs=VMEM,
        scratch_shapes=[
            pltpu.SemaphoreType.DMA((sends,)),
            pltpu.SemaphoreType.DMA((n_sp * n_tp,)),
            pltpu.SemaphoreType.DMA,
        ],
        compiler_params=pltpu.CompilerParams(collective_id=0, has_side_effects=True),
        name="gather_rows",
    )(own)


def moe_kernel(
    n_outer,
    n_inner,
    n_tp,
    chunks,
    tok_ref,
    meta_ref,
    hidden_ref,
    gate_ref,
    up_ref,
    down_ref,
    out_ref,
    tok_all,
    meta_all,
    disp_ref,
    in_ref,
    made_ref,
    back_ref,
    part_ref,
    sum_in,
    gate_all,
    up_all,
    down_all,
    meta_send,
    meta_recv,
    above_send,
    below_send,
    tok_recv,
    disp_send,
    disp_recv,
    back_send,
    back_recv,
    sum_send,
    sum_recv,
    weight_send,
    weight_recv,
):
    sp, tp = lax.axis_index("sp"), lax.axis_index("tp")
    group, member = sp // n_inner, sp % n_inner
    rows = tok_ref.shape[0]
    width = tok_ref.shape[1] // chunks
    slots = disp_ref.shape[2]
    cap = slots // n_inner
    last = n_outer - 1
    has_above, has_below = group < last, group > 0

    def at(plane, place):
        return (plane * n_inner + place, tp)

    others = [at((group + step) % n_outer, member) for step in range(1, n_outer)]
    mates = [(member + step) % n_inner for step in range(1, n_inner)]
    twins = [(sp, (tp + hop) % n_tp) for hop in range(1, n_tp)]
    greet(others + [at(group, mate) for mate in mates] + twins)

    def copy(source, target, send_sem, recv_sem, peer):
        return pltpu.make_async_remote_copy(
            src_ref=source,
            dst_ref=target,
            send_sem=send_sem,
            recv_sem=recv_sem,
            device_id=peer,
            device_id_type=MESH,
        )

    def span(place):
        return pl.ds(pl.multiple_of(place * cap, cap), cap)

    def meta_copy(step):
        return copy(
            meta_ref, meta_all.at[group], meta_send.at[step], meta_recv.at[group], others[step]
        )

    def relay(block, chunk, upward):
        sems = above_send if upward else below_send
        ref = tok_all.at[block, chunk]
        number = block * chunks + chunk
        peer = at(group + 1 if upward else group - 1, member)
        return copy(ref, ref, sems.at[number], tok_recv.at[number], peer)

    def plane_copy(source, target, send_sem, recv_sem, block, chunk, mate):
        number = (block * chunks + chunk) * n_inner
        return copy(
            source.at[block, chunk, span(mate)],
            target.at[block, chunk, span(member)],
            send_sem.at[number + mate],
            recv_sem.at[number + member],
            at(group, mate),
        )

    def disp_copy(block, chunk, mate):
        return plane_copy(disp_ref, in_ref, disp_send, disp_recv, block, chunk, mate)

    def back_copy(block, chunk, mate):
        return plane_copy(made_ref, back_ref, back_send, back_recv, block, chunk, mate)

    def plane_arrived(target, recv_sem, block, chunk):
        for mate in mates:
            arrived(
                target.at[block, chunk, span(mate)],
                recv_sem.at[(block * chunks + chunk) * n_inner + mate],
            )

    def sum_copy(block, chunk, downward):
        slot = jnp.where(downward | (block != group + 1), block, n_outer)
        peer = at(jnp.where(downward, group - 1, group + 1), member)
        return copy(
            part_ref.at[block, chunk],
            sum_in.at[slot, chunk],
            sum_send.at[block * chunks + chunk],
            sum_recv.at[slot * chunks + chunk],
            peer,
        )

    weights = [(gate_ref, gate_all), (up_ref, up_all), (down_ref, down_all)]

    def weight_copies():
        for hop, twin in enumerate(twins):
            for number, (own, everyone) in enumerate(weights):
                slot = hop * 3 + number
                yield copy(
                    own, everyone.at[hop], weight_send.at[slot], weight_recv.at[slot], twin
                )

    first_slot = (group * slots).astype(jnp.float32)

    def named(block):
        numbers = first_slot + lax.broadcasted_iota(jnp.int32, (slots, rows), 0).astype(
            jnp.float32
        )
        meta = meta_all[block]
        return meta[0:1] == numbers, meta[1:2] == numbers, meta

    def scatter(block, chunk):
        one, two, unused = named(block)
        place = jnp.where(one | two, 1.0, 0.0).astype(jnp.bfloat16)
        disp_ref[block, chunk] = jnp.dot(
            place, tok_all[block, chunk], preferred_element_type=jnp.float32
        ).astype(jnp.bfloat16)
        for mate in mates:
            disp_copy(block, chunk, mate).start()
        in_ref[block, chunk, span(member)] = disp_ref[block, chunk, span(member)]

    def expert(block):
        for chunk in range(chunks):
            plane_arrived(in_ref, disp_recv, block, chunk)
        inputs = jnp.concatenate([in_ref[block, chunk] for chunk in range(chunks)], axis=1)
        halves = []
        for hop in range(n_tp):
            gate_half = gate_ref[...] if hop == 0 else gate_all[hop - 1]
            up_half = up_ref[...] if hop == 0 else up_all[hop - 1]
            gate = jnp.dot(inputs, gate_half, preferred_element_type=jnp.float32)
            up = jnp.dot(inputs, up_half, preferred_element_type=jnp.float32)
            halves.append((gate / (1.0 + jnp.exp(-gate)) * up).astype(jnp.bfloat16))
        for chunk in range(chunks):
            columns = slice(chunk * width, (chunk + 1) * width)
            made = jnp.dot(halves[0], down_ref[:, columns], preferred_element_type=jnp.float32)
            for hop in range(1, n_tp):
                made = made + jnp.dot(
                    halves[hop], down_all[hop - 1, :, columns], preferred_element_type=jnp.float32
                )
            made_ref[block, chunk] = made.astype(jnp.bfloat16)
            for mate in mates:
                back_copy(block, chunk, mate).start()
            back_ref[block, chunk, span(member)] = made_ref[block, chunk, span(member)]

    def weighted(block, chunk):
        one, two, meta = named(block)
        shares = jnp.where(one, meta[2:3], 0.0) + jnp.where(two, meta[3:4], 0.0)
        high = shares.astype(jnp.bfloat16)
        low = (shares - high.astype(jnp.float32)).astype(jnp.bfloat16)
        plane_arrived(back_ref, back_recv, block, chunk)
        values = back_ref[block, chunk]
        return lax.dot_general(high, values, TN, preferred_element_type=jnp.float32) + (
            lax.dot_general(low, values, TN, preferred_element_type=jnp.float32)
        )

    def start_sum(block):
        downward = block < group

        @pl.when((downward & (group == last)) | ((block > group) & (group == 0)))
        def _():
            for chunk in range(chunks):
                part_ref[block, chunk] = weighted(block, chunk).astype(jnp.bfloat16)
                sum_copy(block, chunk, downward).start()

    def pass_sum(valid, block, chunk, downward):
        @pl.when(valid)
        def _():
            total = weighted(block, chunk)
            arrived(sum_in.at[block, chunk], sum_recv.at[block * chunks + chunk])
            part_ref[block, chunk] = (
                total + sum_in[block, chunk].astype(jnp.float32)
            ).astype(jnp.bfloat16)
            sum_copy(block, chunk, downward).start()

    def both(distance, action):
        @pl.when(group >= distance)
        def _():
            action(group - distance)

        @pl.when((distance > 0) & (group + distance < n_outer))
        def _():
            action(group + distance)

    meta_all[group] = meta_ref[...]
    for step in range(n_outer - 1):
        meta_copy(step).start()
    for chunk in range(chunks):
        tok_all[group, chunk] = tok_ref[:, chunk * width : (chunk + 1) * width]

        @pl.when(has_above)
        def _():
            relay(group, chunk, True).start()

        @pl.when(has_below)
        def _():
            relay(group, chunk, False).start()

    for item in weight_copies():
        item.start()
    for chunk in range(chunks):
        scatter(group, chunk)

    def receive(block, chunk, upward):
        number = block * chunks + chunk
        arrived(tok_all.at[block, chunk], tok_recv.at[number])
        if chunk == 0:
            arrived(meta_all.at[block], meta_recv.at[block])

        @pl.when(has_above if upward else has_below)
        def _():
            relay(block, chunk, upward).start()

        scatter(block, chunk)

    def stage(distance, carry):
        for chunk in range(chunks):

            @pl.when(group >= distance)
            def _():
                receive(group - distance, chunk, True)

            @pl.when(group + distance < n_outer)
            def _():
                receive(group + distance, chunk, False)

            if chunk == EXPERT_LAG % chunks:

                @pl.when(distance == 1)
                def _():
                    for item in weight_copies():
                        item.wait_recv()

                both(distance - 1, expert)
            if chunk == SUM_LAG % chunks:
                both(distance - 1, start_sum)
        return carry

    lax.fori_loop(1, n_outer, stage, 0)
    both(last, expert)
    both(last, start_sum)

    def sum_stage(distance, carry):
        low_first = 2 * group >= n_outer
        low, high = last - distance, distance + 0
        low_valid = (low < group) & has_above
        high_valid = (high > group) & has_below
        first = jnp.where(low_first, low, high)
        second = jnp.where(low_first, high, low)
        first_valid = (low_first & low_valid) | (jnp.logical_not(low_first) & high_valid)
        second_valid = (low_first & high_valid) | (jnp.logical_not(low_first) & low_valid)
        lag = chunks // 2
        for step in range(chunks + lag):
            if step < chunks:
                pass_sum(first_valid, first, step, first < group)
            if step >= lag:
                pass_sum(second_valid, second, step - lag, second < group)
        return carry

    lax.fori_loop(1, n_outer, sum_stage, 0)

    for chunk in range(chunks):
        columns = slice(chunk * width, (chunk + 1) * width)
        total = weighted(group, chunk) + hidden_ref[:, columns].astype(jnp.float32)
        sides = []
        for side, slot in ((has_above, group), (has_below, n_outer)):

            @pl.when(side)
            def _(slot=slot):
                arrived(sum_in.at[slot, chunk], sum_recv.at[slot * chunks + chunk])

            sides.append(
                jnp.where(side, sum_in[slot, chunk].astype(jnp.float32), 0.0)
            )
        out_ref[:, columns] = (total + sides[0] + sides[1]).astype(out_ref.dtype)

    for step in range(n_outer - 1):
        meta_copy(step).wait_send()
    for item in weight_copies():
        item.wait_send()

    def drain(block, carry):
        for chunk in range(chunks):

            @pl.when(has_above & (block <= group))
            def _():
                relay(block, chunk, True).wait_send()

            @pl.when(has_below & (block >= group))
            def _():
                relay(block, chunk, False).wait_send()

            for mate in mates:
                disp_copy(block, chunk, mate).wait_send()
                back_copy(block, chunk, mate).wait_send()

            @pl.when(block != group)
            def _():
                sum_copy(block, chunk, block < group).wait_send()

        return carry

    lax.fori_loop(0, n_outer, drain, 0)


EXPERT_LAG = 0
SUM_LAG = 1
TN = (((0,), (0,)), ((), ()))


def moe(tokens, meta, hidden, gate, up, down, n_sp, n_tp, cap):
    n_inner = math.gcd(n_sp, 4)
    n_outer = n_sp // n_inner
    rows, width = tokens.shape
    chunks = math.gcd(width // 128, 4)
    part = width // chunks
    slots = n_inner * cap
    dma = pltpu.SemaphoreType.DMA
    vmem = pltpu.VMEM
    blocks = n_outer * chunks
    low = jnp.bfloat16
    return pl.pallas_call(
        functools.partial(moe_kernel, n_outer, n_inner, n_tp, chunks),
        out_shape=jax.ShapeDtypeStruct((rows, width), low),
        in_specs=[VMEM] * 6,
        out_specs=VMEM,
        scratch_shapes=[
            vmem((n_outer, chunks, rows, part), low),
            vmem((n_outer,) + meta.shape, meta.dtype),
            vmem((n_outer, chunks, slots, part), low),
            vmem((n_outer, chunks, slots, part), low),
            vmem((n_outer, chunks, slots, part), low),
            vmem((n_outer, chunks, slots, part), low),
            vmem((n_outer, chunks, rows, part), low),
            vmem((n_outer + 1, chunks, rows, part), low),
            vmem((n_tp - 1,) + gate.shape, low),
            vmem((n_tp - 1,) + up.shape, low),
            vmem((n_tp - 1,) + down.shape, low),
            dma((n_outer - 1,)),
            dma((n_outer,)),
            dma((blocks,)),
            dma((blocks,)),
            dma((blocks,)),
            dma((blocks * n_inner,)),
            dma((blocks * n_inner,)),
            dma((blocks * n_inner,)),
            dma((blocks * n_inner,)),
            dma((blocks,)),
            dma((blocks + chunks,)),
            dma((3 * (n_tp - 1),)),
            dma((3 * (n_tp - 1),)),
        ],
        compiler_params=pltpu.CompilerParams(
            collective_id=1, has_side_effects=True, vmem_limit_bytes=67043328
        ),
        name="experts",
    )(tokens, meta, hidden, gate, up, down)


def heads_kernel(n_tp, own_ref, out_ref, send_sem, recv_sem, local_sem):
    sp, tp = lax.axis_index("sp"), lax.axis_index("tp")
    twins = [(sp, (tp + hop) % n_tp) for hop in range(1, n_tp)]
    greet(twins)
    rows = out_ref.shape[1]

    def part(core):
        return own_ref.at[pl.ds(pl.multiple_of(core * rows, rows), rows)]

    copies = [
        send(part(twin[1]), out_ref.at[tp], send_sem.at[hop], recv_sem.at[tp], twin)
        for hop, twin in enumerate(twins)
    ]
    keep = pltpu.make_async_copy(part(tp), out_ref.at[tp], local_sem)
    keep.start()
    for twin in twins:
        arrived(out_ref.at[twin[1]], recv_sem.at[twin[1]])
    keep.wait()
    for copy in copies:
        copy.wait_send()


def swap_heads(own, n_tp):
    return pl.pallas_call(
        functools.partial(heads_kernel, n_tp),
        out_shape=jax.ShapeDtypeStruct((n_tp, own.shape[0] // n_tp, own.shape[1]), own.dtype),
        in_specs=[VMEM],
        out_specs=VMEM,
        scratch_shapes=[
            pltpu.SemaphoreType.DMA((n_tp - 1,)),
            pltpu.SemaphoreType.DMA((n_tp,)),
            pltpu.SemaphoreType.DMA,
        ],
        compiler_params=pltpu.CompilerParams(collective_id=2, has_side_effects=True),
        name="swap_heads",
    )(own)


NT = (((1,), (1,)), ((), ()))


def attention_kernel(
    key_block, latent_width, heads, base_ref, query_ref, kv_ref, key_up_ref, value_up_ref, out_ref, max_ref, sum_ref, acc_ref
):
    first = base_ref[0]
    queries = query_ref.shape[2]
    scale = (QK_NOPE + QK_ROPE) ** (-0.5) * math.log2(math.e)
    max_ref[...] = jnp.full_like(max_ref, NEG_LARGE)
    sum_ref[...] = jnp.zeros_like(sum_ref)
    acc_ref[...] = jnp.zeros_like(acc_ref)

    def block(start, masked):
        start = pl.multiple_of(start, key_block)
        rows = kv_ref[pl.ds(start, key_block), :]
        latent = rows[:, :latent_width]
        rot = rows[:, latent_width:]
        keys = jnp.dot(latent, key_up_ref[...], preferred_element_type=jnp.float32).astype(
            jnp.bfloat16
        )
        values = lax.dot_general(
            value_up_ref[...], latent, NT, preferred_element_type=jnp.float32
        ).astype(jnp.bfloat16)
        if masked:
            key_segment = (
                start + lax.broadcasted_iota(jnp.int32, (key_block, queries), 0)
            ) // SEGMENT
            query_segment = (
                first + lax.broadcasted_iota(jnp.int32, (key_block, queries), 1)
            ) // SEGMENT
            allowed = key_segment <= query_segment
        for head in range(heads):
            wide = jnp.concatenate([keys[:, head * QK_NOPE : (head + 1) * QK_NOPE], rot], axis=1)
            scores = jnp.dot(wide, query_ref[head], preferred_element_type=jnp.float32)
            if masked:
                scores = jnp.where(allowed, scores, NEG_LARGE)
            old_max = max_ref[head]
            new_max = jnp.maximum(old_max, jnp.max(scores, axis=0, keepdims=True))
            weights = jnp.exp2((scores - new_max) * scale)
            shrink = jnp.exp2((old_max - new_max) * scale)
            max_ref[head] = new_max
            sum_ref[head] = sum_ref[head] * shrink + jnp.sum(weights, axis=0, keepdims=True)
            acc_ref[head] = acc_ref[head] * shrink + jnp.dot(
                values[head * V_DIM : (head + 1) * V_DIM],
                weights.astype(jnp.bfloat16),
                preferred_element_type=jnp.float32,
            )

    whole = first // key_block

    def body(step, carry):
        block(step * key_block, False)
        return carry

    lax.fori_loop(0, whole, body, 0)
    block(whole * key_block, True)
    for head in range(heads):
        out_ref[:, head * V_DIM : (head + 1) * V_DIM] = (
            (acc_ref[head] / sum_ref[head]).T.astype(out_ref.dtype)
        )


def attention(base, query, kv, key_up, value_up_t, key_block, latent_width):
    heads, unused, queries = query.shape
    return pl.pallas_call(
        functools.partial(attention_kernel, key_block, latent_width, heads),
        out_shape=jax.ShapeDtypeStruct((queries, heads * V_DIM), jnp.bfloat16),
        in_specs=[pl.BlockSpec(memory_space=pltpu.SMEM), VMEM, VMEM, VMEM, VMEM],
        out_specs=VMEM,
        scratch_shapes=[
            pltpu.VMEM((heads, 1, queries), jnp.float32),
            pltpu.VMEM((heads, 1, queries), jnp.float32),
            pltpu.VMEM((heads, V_DIM, queries), jnp.float32),
        ],
        name="attention",
    )(base, query, kv, key_up, value_up_t)


def local(
    residual,
    query_nope,
    query_rope,
    latent,
    key_rope,
    key_up,
    value_up,
    out_proj,
    norm_gain,
    routes,
    route_weight,
    w_gate,
    w_up,
    w_down,
):
    tp_count = lax.axis_size("tp")
    sp_count = lax.axis_size("sp")
    tp_index = lax.axis_index("tp")
    sp_index = lax.axis_index("sp")
    row_count = residual.shape[0]
    tok_dev = query_nope.shape[0]
    heads_here = query_nope.shape[1] // QK_NOPE
    query_first = sp_index * tok_dev
    query_pos = query_first + jnp.arange(tok_dev, dtype=jnp.int32)
    query_rot = rotary(
        query_rope.astype(jnp.float32).reshape(tok_dev, heads_here, QK_ROPE), query_pos
    ).astype(jnp.bfloat16)
    query_heads = query_nope.reshape(tok_dev, heads_here, QK_NOPE)
    key_pos = query_first + tp_index * row_count + jnp.arange(row_count, dtype=jnp.int32)
    key_rot = rotary(key_rope.astype(jnp.float32), key_pos).astype(jnp.bfloat16)
    width_pad = -(-QK_ROPE // 128) * 128 - QK_ROPE
    packed = jnp.concatenate(
        [latent, key_rot, jnp.zeros((row_count, width_pad), jnp.bfloat16)], axis=1
    )
    gathered = gather_rows(packed, sp_count, tp_count)
    kv_rows = gathered.reshape(sp_count * tok_dev, packed.shape[1])
    query = jnp.concatenate(
        [query_heads, query_rot, jnp.zeros((tok_dev, heads_here, width_pad), jnp.bfloat16)], axis=2
    ).transpose(1, 2, 0)
    key_block = tok_dev * math.gcd(sp_count, 2)
    attn_out = attention(
        query_first.astype(jnp.int32).reshape(1),
        query,
        kv_rows,
        key_up,
        value_up.T,
        key_block,
        latent.shape[1],
    )
    all_heads = swap_heads(attn_out, tp_count)
    proj_parts = out_proj.reshape(tp_count, attn_out.shape[1], out_proj.shape[1])
    projected = jnp.dot(all_heads[0], proj_parts[0], preferred_element_type=jnp.float32)
    for core in range(1, tp_count):
        projected = projected + jnp.dot(
            all_heads[core], proj_parts[core], preferred_element_type=jnp.float32
        )
    hidden_wide = residual.astype(jnp.float32) + projected
    hidden = hidden_wide.astype(jnp.bfloat16)
    hidden_wide = hidden.astype(jnp.float32)
    normed = hidden_wide * lax.rsqrt(
        jnp.mean(hidden_wide * hidden_wide, axis=-1, keepdims=True) + EPSILON
    )
    normed = (normed * norm_gain[None, :]).astype(jnp.bfloat16)
    expert_count = lax.axis_size("sp")
    capacity = max(2, 2 * (row_count * tp_count) // expert_count)
    capacity = -(-capacity // 16) * 16
    top_count = routes.shape[1]
    flat_expert = routes.reshape(-1)
    onehot = (flat_expert[:, None] == jnp.arange(expert_count, dtype=jnp.int32)[None, :]).astype(
        jnp.int32
    )
    slot_rank = jnp.sum(jnp.cumsum(onehot, axis=0) * onehot, axis=1) - 1
    slot_index = flat_expert * capacity + slot_rank
    slots = slot_index.reshape(row_count, top_count).astype(jnp.float32)
    meta = jnp.concatenate(
        [slots.T, route_weight.T, jnp.zeros((8 - 2 * top_count, row_count), jnp.float32)], axis=0
    )
    return moe(
        normed, meta, hidden, w_gate[0], w_up[0], w_down[0], sp_count, tp_count, capacity
    )


def solution(mesh):
    return jax.shard_map(
        local,
        mesh=mesh,
        in_specs=(
            P(("sp", "tp"), None),
            P("sp", "tp"),
            P("sp", "tp"),
            P(("sp", "tp"), None),
            P(("sp", "tp"), None),
            P(None, "tp"),
            P(None, "tp"),
            P(),
            P(),
            P(("sp", "tp"), None),
            P(("sp", "tp"), None),
            P("sp", None, "tp"),
            P("sp", None, "tp"),
            P("sp", "tp", None),
        ),
        out_specs=P(("sp", "tp"), None),
        check_vma=False,
    )
```

```python
import functools
import math

import jax
import jax.numpy as jnp
from jax import lax
from jax.experimental import pallas as pl
from jax.experimental.pallas import tpu as pltpu
from jax.sharding import PartitionSpec as P

QK_NOPE = 128
QK_ROPE = 64
V_DIM = 128
SEGMENT = 64


EPSILON = 1e-06
ROPE_BASE = 10000.0
NEG_LARGE = -1e30


MESH = pl.DeviceIdType.MESH
VMEM = pl.BlockSpec(memory_space=pltpu.VMEM)


def greet(peers):
    barrier = pltpu.get_barrier_semaphore()
    for peer in peers:
        pl.semaphore_signal(barrier, inc=1, device_id=peer, device_id_type=MESH)
    pl.semaphore_wait(barrier, len(peers))


def arrived(block, semaphore):
    pltpu.make_async_copy(block, block, semaphore).wait()


def attend_kernel(
    n_outer,
    n_inner,
    n_tp,
    table_ref,
    nope_ref,
    rope_ref,
    latent_ref,
    key_rope_ref,
    key_up_ref,
    value_up_ref,
    residual_ref,
    gain_ref,
    proj_hbm,
    hidden_ref,
    normed_ref,
    kv_ref,
    query_ref,
    value_ref,
    max_ref,
    sum_ref,
    acc_ref,
    own_ref,
    heads_ref,
    proj_ref,
    plane_send,
    mate_send,
    twin_send,
    kv_recv,
    heads_send,
    heads_recv,
    proj_sem,
):
    sp, tp = lax.axis_index("sp"), lax.axis_index("tp")
    group, member = sp // n_inner, sp % n_inner
    queries = nope_ref.shape[0]
    rows, latent_width = latent_ref.shape
    heads = nope_ref.shape[1] // QK_NOPE
    packed = rows // (latent_width // QK_ROPE)
    scale = (QK_NOPE + QK_ROPE) ** (-0.5) * math.log2(math.e)
    twins = [(tp + hop) % n_tp for hop in range(1, n_tp)]
    mates = [(member + step) % n_inner for step in range(n_inner)]

    load = pltpu.make_async_copy(proj_hbm, proj_ref, proj_sem)
    load.start()

    def copy(source, target, send_sem, recv_sem, peer):
        return pltpu.make_async_remote_copy(
            src_ref=source,
            dst_ref=target,
            send_sem=send_sem,
            recv_sem=recv_sem,
            device_id=peer,
            device_id_type=MESH,
        )

    def kv_copy(block, send_sem, peer):
        ref = kv_ref.at[block, tp]
        return copy(ref, ref, send_sem, kv_recv.at[block * n_tp + tp], peer)

    def plane_copy(step):
        return kv_copy(sp, plane_send.at[step], ((group + step) * n_inner + member, tp))

    def mate_copy(distance, step):
        return kv_copy(
            (group - distance) * n_inner + member,
            mate_send.at[distance * n_inner + step],
            (group * n_inner + mates[step], tp),
        )

    def twin_copies(block):
        return [
            kv_copy(block, twin_send.at[block * (n_tp - 1) + hop], (sp, twin))
            for hop, twin in enumerate(twins)
        ]

    def landed(block, core):
        arrived(kv_ref.at[block, core], kv_recv.at[block * n_tp + core])

    lane = lax.broadcasted_iota(jnp.int32, (1, 2 * QK_ROPE), 1)
    early = lane % QK_ROPE < QK_ROPE // 2

    def rotated(values, first):
        where = pl.ds(pl.multiple_of(first, values.shape[0]), values.shape[0])
        values = values.astype(jnp.float32)
        swapped = jnp.where(
            early,
            pltpu.roll(values, 2 * QK_ROPE - QK_ROPE // 2, 1),
            pltpu.roll(values, QK_ROPE // 2, 1),
        )
        return values * table_ref[0, where] + swapped * table_ref[1, where]

    wide_rope = jnp.concatenate([key_rope_ref[...]] * 2, axis=1)
    key_rot = rotated(wide_rope, tp * rows)
    kv_ref[sp, tp, :rows] = latent_ref[...]
    for pair in range(latent_width // (2 * QK_ROPE)):
        low = key_rot[(2 * pair) * packed : (2 * pair + 1) * packed]
        high = key_rot[(2 * pair + 1) * packed : (2 * pair + 2) * packed]
        kv_ref[sp, tp, rows:, pair * 2 * QK_ROPE : (pair + 1) * 2 * QK_ROPE] = jnp.where(
            lane < QK_ROPE, low, high
        ).astype(jnp.bfloat16)

    planes = [((group + step) % n_outer * n_inner + member, tp) for step in range(1, n_outer)]
    greet(
        planes
        + [(group * n_inner + mate, tp) for mate in mates[1:]]
        + [(sp, twin) for twin in twins]
    )

    for item in twin_copies(sp):
        item.start()
    for step in range(1, max(n_inner, n_outer)):
        if step < n_outer:

            @pl.when(group + step < n_outer)
            def _():
                plane_copy(step).start()

        if step < n_inner:

            @pl.when(mates[step] > member)
            def _():
                mate_copy(0, step).start()

    for pair in range(0, heads, 2):
        both = rotated(rope_ref[:, pair * QK_ROPE : (pair + 2) * QK_ROPE], 0).T
        for head in (pair, pair + 1):
            columns = slice(head * QK_NOPE, (head + 1) * QK_NOPE)
            query_ref[head, :QK_NOPE] = nope_ref[:, columns].astype(jnp.float32).T.astype(
                jnp.bfloat16
            )
            query_ref[head, QK_NOPE : QK_NOPE + QK_ROPE] = both[
                (head - pair) * QK_ROPE : (head - pair + 1) * QK_ROPE
            ].astype(jnp.bfloat16)
            query_ref[head, QK_NOPE + QK_ROPE :] = jnp.zeros(
                (QK_ROPE, queries), jnp.bfloat16
            )
    value_ref[...] = value_up_ref[...].astype(jnp.float32).T.astype(jnp.bfloat16)

    def attend(blocks, own):
        latents, rots = [], []
        for block in blocks:
            for core in range(n_tp):
                latents.append(kv_ref[block, core, :rows])
                for pair in range(latent_width // (2 * QK_ROPE)):
                    part = kv_ref[
                        block, core, rows:, pair * 2 * QK_ROPE : (pair + 1) * 2 * QK_ROPE
                    ].astype(jnp.float32)
                    rots.append(part.astype(jnp.bfloat16))
                    rots.append(pltpu.roll(part, QK_ROPE, 1).astype(jnp.bfloat16))
        latent = jnp.concatenate(latents, axis=0)
        rot = jnp.concatenate(rots, axis=0)
        count = latent.shape[0]
        keys = jnp.dot(latent, key_up_ref[...], preferred_element_type=jnp.float32).astype(
            jnp.bfloat16
        )
        values = lax.dot_general(
            value_ref[...], latent, NT, preferred_element_type=jnp.float32
        ).astype(jnp.bfloat16)
        if own:
            allowed = (
                lax.broadcasted_iota(jnp.int32, (count, queries), 0) // SEGMENT
                <= lax.broadcasted_iota(jnp.int32, (count, queries), 1) // SEGMENT
            )
        for head in range(heads):
            wide = jnp.concatenate([keys[:, head * QK_NOPE : (head + 1) * QK_NOPE], rot], axis=1)
            scores = jnp.dot(wide, query_ref[head], preferred_element_type=jnp.float32)
            if own:
                scores = jnp.where(allowed, scores, NEG_LARGE)
            new_max = jnp.max(scores, axis=0, keepdims=True)
            if not own:
                old_max = max_ref[head]
                new_max = jnp.maximum(old_max, new_max)
                shrink = jnp.exp2((old_max - new_max) * scale)
            weights = jnp.exp2((scores - new_max) * scale)
            total = jnp.sum(weights, axis=0, keepdims=True)
            product = jnp.dot(
                values[head * V_DIM : (head + 1) * V_DIM],
                weights.astype(jnp.bfloat16),
                preferred_element_type=jnp.float32,
            )
            max_ref[head] = new_max
            if own:
                sum_ref[head] = total
                acc_ref[head] = product
            else:
                sum_ref[head] = sum_ref[head] * shrink + total
                acc_ref[head] = acc_ref[head] * shrink + product

    def from_plane(distance):
        block = (group - distance) * n_inner + member
        landed(block, tp)
        for step in range(1, n_inner):
            mate_copy(distance, step).start()
        for item in twin_copies(block):
            item.start()

    def from_mate(distance, step):
        block = (group - distance) * n_inner + mates[step]
        landed(block, tp)
        for item in twin_copies(block):
            item.start()

    def ready(distance, step):
        block = (group - distance) * n_inner + mates[step]
        for twin in twins:
            landed(block, twin)
        return block

    attend([ready(0, 0)], True)

    @pl.when(group >= 1)
    def _():
        from_plane(1)

    for step in range(1, n_inner):

        @pl.when(mates[step] < member)
        def _():
            from_mate(0, step)

    @pl.when(group >= 2)
    def _():
        from_plane(2)

    def inside(step, carry):
        mate = (member + step) % n_inner

        @pl.when(mate < member)
        def _():
            block = group * n_inner + mate
            for twin in twins:
                landed(block, twin)
            attend([block], False)

        return carry

    lax.fori_loop(1, n_inner, inside, 0)

    def outside(distance, carry):
        @pl.when(distance + 2 <= group)
        def _():
            from_plane(distance + 2)

        unit = 2 if n_inner % 2 == 0 else 1
        for first in range(0, n_inner, unit):
            for step in range(first, first + unit):
                if step > 0:
                    from_mate(distance, step)
            attend([ready(distance, step) for step in range(first, first + unit)], False)
        return carry

    lax.fori_loop(1, group + 1, outside, 0)

    def heads_copy(hop):
        return copy(
            own_ref.at[pl.ds(pl.multiple_of(twins[hop] * rows, rows), rows)],
            heads_ref.at[hop],
            heads_send.at[hop],
            heads_recv.at[hop],
            (sp, twins[hop]),
        )

    for head in range(heads):
        own_ref[:, head * V_DIM : (head + 1) * V_DIM] = (
            (acc_ref[head] / sum_ref[head]).T.astype(own_ref.dtype)
        )
    for hop in range(n_tp - 1):
        heads_copy(hop).start()
    load.wait()
    depth = heads * V_DIM
    width = residual_ref.shape[1]
    part = width // math.gcd(width // 128, 4)

    def proj(core, columns):
        return proj_ref[pl.ds(pl.multiple_of(core * depth, depth), depth), columns]

    mine = own_ref[pl.ds(pl.multiple_of(tp * rows, rows), rows)]
    spans = [slice(first, first + part) for first in range(0, width, part)]
    sums = []
    for columns in spans:
        sums.append(
            residual_ref[:, columns].astype(jnp.float32)
            + jnp.dot(mine, proj(tp, columns), preferred_element_type=jnp.float32)
        )
    for hop in range(n_tp - 1):
        arrived(heads_ref.at[hop], heads_recv.at[hop])
        for number, columns in enumerate(spans):
            sums[number] = sums[number] + jnp.dot(
                heads_ref[hop], proj((tp + n_tp - hop - 1) % n_tp, columns),
                preferred_element_type=jnp.float32,
            )
    square = jnp.zeros((rows, 1), jnp.float32)
    for number, columns in enumerate(spans):
        hidden = sums[number].astype(jnp.bfloat16)
        hidden_ref[:, columns] = hidden
        hidden = hidden.astype(jnp.float32)
        square = square + jnp.sum(hidden * hidden, axis=1, keepdims=True)
    factor = lax.rsqrt(square / width + EPSILON)
    for columns in spans:
        normed_ref[:, columns] = (
            hidden_ref[:, columns].astype(jnp.float32) * factor * gain_ref[:, columns]
        ).astype(jnp.bfloat16)

    for hop in range(n_tp - 1):
        heads_copy(hop).wait_send()
    for item in twin_copies(sp):
        item.wait_send()
    for step in range(1, n_outer):

        @pl.when(group + step < n_outer)
        def _():
            plane_copy(step).wait_send()

    for step in range(1, n_inner):

        @pl.when(mates[step] > member)
        def _():
            mate_copy(0, step).wait_send()

        @pl.when(mates[step] < member)
        def _():
            for item in twin_copies(group * n_inner + mates[step]):
                item.wait_send()

    def drain(distance, carry):
        for step in range(n_inner):
            if step > 0:
                mate_copy(distance, step).wait_send()
            for item in twin_copies((group - distance) * n_inner + mates[step]):
                item.wait_send()
        return carry

    lax.fori_loop(1, group + 1, drain, 0)


NT = (((1,), (1,)), ((), ()))


def attend(
    table, nope, rope, latent, key_rope, key_up, value_up, residual, gain, proj, n_sp, n_tp
):
    n_inner = math.gcd(n_sp, 4)
    n_outer = n_sp // n_inner
    queries = nope.shape[0]
    heads = nope.shape[1] // QK_NOPE
    rows, latent_width = latent.shape
    packed = rows // (latent_width // QK_ROPE)
    dma = pltpu.SemaphoreType.DMA
    vmem = pltpu.VMEM
    low, wide = jnp.bfloat16, jnp.float32
    return pl.pallas_call(
        functools.partial(attend_kernel, n_outer, n_inner, n_tp),
        out_shape=[jax.ShapeDtypeStruct(residual.shape, low)] * 2,
        in_specs=[VMEM] * 9 + [pl.BlockSpec(memory_space=pl.ANY)],
        out_specs=[VMEM] * 2,
        scratch_shapes=[
            vmem((n_sp, n_tp, rows + packed, latent_width), low),
            vmem((heads, QK_NOPE + 2 * QK_ROPE, queries), low),
            vmem((heads * V_DIM, latent_width), low),
            vmem((heads, 1, queries), wide),
            vmem((heads, 1, queries), wide),
            vmem((heads, V_DIM, queries), wide),
            vmem((queries, heads * V_DIM), low),
            vmem((n_tp - 1, rows, heads * V_DIM), low),
            vmem(proj.shape, low),
            dma((n_outer,)),
            dma((n_sp,)),
            dma((n_sp * (n_tp - 1),)),
            dma((n_sp * n_tp,)),
            dma((n_tp - 1,)),
            dma((n_tp - 1,)),
            dma,
        ],
        compiler_params=pltpu.CompilerParams(
            collective_id=0, has_side_effects=True, vmem_limit_bytes=48 * 2**20
        ),
        name="attend",
    )(table, nope, rope, latent, key_rope, key_up, value_up, residual, gain, proj)


def moe_kernel(
    n_outer,
    n_inner,
    n_tp,
    chunks,
    tok_ref,
    meta_ref,
    hidden_ref,
    gate_ref,
    up_ref,
    down_ref,
    out_ref,
    tok_all,
    meta_all,
    disp_ref,
    in_ref,
    made_ref,
    back_ref,
    part_ref,
    sum_in,
    gate_all,
    up_all,
    down_all,
    meta_send,
    meta_recv,
    above_send,
    below_send,
    tok_recv,
    disp_send,
    disp_recv,
    back_send,
    back_recv,
    sum_send,
    sum_recv,
    weight_send,
    weight_recv,
):
    sp, tp = lax.axis_index("sp"), lax.axis_index("tp")
    group, member = sp // n_inner, sp % n_inner
    rows = tok_ref.shape[0]
    width = tok_ref.shape[1] // chunks
    slots = disp_ref.shape[2]
    cap = slots // n_inner
    last = n_outer - 1
    has_above, has_below = group < last, group > 0

    def at(plane, place):
        return (plane * n_inner + place, tp)

    others = [at((group + step) % n_outer, member) for step in range(1, n_outer)]
    mates = [(member + step) % n_inner for step in range(1, n_inner)]
    twins = [(sp, (tp + hop) % n_tp) for hop in range(1, n_tp)]
    greet(others + [at(group, mate) for mate in mates] + twins)

    def copy(source, target, send_sem, recv_sem, peer):
        return pltpu.make_async_remote_copy(
            src_ref=source,
            dst_ref=target,
            send_sem=send_sem,
            recv_sem=recv_sem,
            device_id=peer,
            device_id_type=MESH,
        )

    def span(place):
        return pl.ds(pl.multiple_of(place * cap, cap), cap)

    def meta_copy(step):
        return copy(
            meta_ref, meta_all.at[group], meta_send.at[step], meta_recv.at[group], others[step]
        )

    def relay(block, chunk, upward):
        sems = above_send if upward else below_send
        ref = tok_all.at[block, chunk]
        number = block * chunks + chunk
        peer = at(group + 1 if upward else group - 1, member)
        return copy(ref, ref, sems.at[number], tok_recv.at[number], peer)

    def plane_copy(source, target, send_sem, recv_sem, block, chunk, mate):
        number = (block * chunks + chunk) * n_inner
        return copy(
            source.at[block, chunk, span(mate)],
            target.at[block, chunk, span(member)],
            send_sem.at[number + mate],
            recv_sem.at[number + member],
            at(group, mate),
        )

    def disp_copy(block, chunk, mate):
        return plane_copy(disp_ref, in_ref, disp_send, disp_recv, block, chunk, mate)

    def back_copy(block, chunk, mate):
        return plane_copy(made_ref, back_ref, back_send, back_recv, block, chunk, mate)

    def plane_arrived(target, recv_sem, block, chunk):
        for mate in mates:
            arrived(
                target.at[block, chunk, span(mate)],
                recv_sem.at[(block * chunks + chunk) * n_inner + mate],
            )

    def sum_copy(block, chunk, downward):
        slot = jnp.where(downward | (block != group + 1), block, n_outer)
        peer = at(jnp.where(downward, group - 1, group + 1), member)
        return copy(
            part_ref.at[block, chunk],
            sum_in.at[slot, chunk],
            sum_send.at[block * chunks + chunk],
            sum_recv.at[slot * chunks + chunk],
            peer,
        )

    weights = [(gate_ref, gate_all), (up_ref, up_all), (down_ref, down_all)]

    def weight_copies():
        for hop, twin in enumerate(twins):
            for number, (own, everyone) in enumerate(weights):
                slot = hop * 3 + number
                yield copy(
                    own, everyone.at[hop], weight_send.at[slot], weight_recv.at[slot], twin
                )

    first_slot = (group * slots).astype(jnp.float32)

    def named(block):
        numbers = first_slot + lax.broadcasted_iota(jnp.int32, (slots, rows), 0).astype(
            jnp.float32
        )
        meta = meta_all[block]
        return meta[0:1] == numbers, meta[1:2] == numbers, meta

    def scatter(block, chunk):
        one, two, unused = named(block)
        place = jnp.where(one | two, 1.0, 0.0).astype(jnp.bfloat16)
        disp_ref[block, chunk] = jnp.dot(
            place, tok_all[block, chunk], preferred_element_type=jnp.float32
        ).astype(jnp.bfloat16)
        for mate in mates:
            disp_copy(block, chunk, mate).start()
        in_ref[block, chunk, span(member)] = disp_ref[block, chunk, span(member)]

    def expert(block):
        for chunk in range(chunks):
            plane_arrived(in_ref, disp_recv, block, chunk)
        inputs = jnp.concatenate([in_ref[block, chunk] for chunk in range(chunks)], axis=1)
        halves = []
        for hop in range(n_tp):
            gate_half = gate_ref[...] if hop == 0 else gate_all[hop - 1]
            up_half = up_ref[...] if hop == 0 else up_all[hop - 1]
            gate = jnp.dot(inputs, gate_half, preferred_element_type=jnp.float32)
            up = jnp.dot(inputs, up_half, preferred_element_type=jnp.float32)
            halves.append((gate / (1.0 + jnp.exp(-gate)) * up).astype(jnp.bfloat16))
        for chunk in range(chunks):
            columns = slice(chunk * width, (chunk + 1) * width)
            made = jnp.dot(halves[0], down_ref[:, columns], preferred_element_type=jnp.float32)
            for hop in range(1, n_tp):
                made = made + jnp.dot(
                    halves[hop], down_all[hop - 1, :, columns], preferred_element_type=jnp.float32
                )
            made_ref[block, chunk] = made.astype(jnp.bfloat16)
            for mate in mates:
                back_copy(block, chunk, mate).start()
            back_ref[block, chunk, span(member)] = made_ref[block, chunk, span(member)]

    def weighted(block, chunk):
        one, two, meta = named(block)
        shares = jnp.where(one, meta[2:3], 0.0) + jnp.where(two, meta[3:4], 0.0)
        high = shares.astype(jnp.bfloat16)
        low = (shares - high.astype(jnp.float32)).astype(jnp.bfloat16)
        plane_arrived(back_ref, back_recv, block, chunk)
        values = back_ref[block, chunk]
        return lax.dot_general(high, values, TN, preferred_element_type=jnp.float32) + (
            lax.dot_general(low, values, TN, preferred_element_type=jnp.float32)
        )

    def start_sum(block):
        downward = block < group

        @pl.when((downward & (group == last)) | ((block > group) & (group == 0)))
        def _():
            for chunk in range(chunks):
                part_ref[block, chunk] = weighted(block, chunk).astype(jnp.bfloat16)
                sum_copy(block, chunk, downward).start()

    def pass_sum(valid, block, chunk, downward):
        @pl.when(valid)
        def _():
            total = weighted(block, chunk)
            arrived(sum_in.at[block, chunk], sum_recv.at[block * chunks + chunk])
            part_ref[block, chunk] = (
                total + sum_in[block, chunk].astype(jnp.float32)
            ).astype(jnp.bfloat16)
            sum_copy(block, chunk, downward).start()

    def both(distance, action):
        @pl.when(group >= distance)
        def _():
            action(group - distance)

        @pl.when((distance > 0) & (group + distance < n_outer))
        def _():
            action(group + distance)

    meta_all[group] = meta_ref[...]
    for step in range(n_outer - 1):
        meta_copy(step).start()
    for chunk in range(chunks):
        tok_all[group, chunk] = tok_ref[:, chunk * width : (chunk + 1) * width]

        @pl.when(has_above)
        def _():
            relay(group, chunk, True).start()

        @pl.when(has_below)
        def _():
            relay(group, chunk, False).start()

    for item in weight_copies():
        item.start()
    for chunk in range(chunks):
        scatter(group, chunk)

    def receive(block, chunk, upward):
        number = block * chunks + chunk
        arrived(tok_all.at[block, chunk], tok_recv.at[number])
        if chunk == 0:
            arrived(meta_all.at[block], meta_recv.at[block])

        @pl.when(has_above if upward else has_below)
        def _():
            relay(block, chunk, upward).start()

        scatter(block, chunk)

    def stage(distance, carry):
        for chunk in range(chunks):

            @pl.when(group >= distance)
            def _():
                receive(group - distance, chunk, True)

            @pl.when(group + distance < n_outer)
            def _():
                receive(group + distance, chunk, False)

            if chunk == EXPERT_LAG % chunks:

                @pl.when(distance == 1)
                def _():
                    for item in weight_copies():
                        item.wait_recv()

                both(distance - 1, expert)
            if chunk == SUM_LAG % chunks:
                both(distance - 1, start_sum)
        return carry

    lax.fori_loop(1, n_outer, stage, 0)
    both(last, expert)
    both(last, start_sum)

    def sum_stage(distance, carry):
        low_first = 2 * group >= n_outer
        low, high = last - distance, distance + 0
        low_valid = (low < group) & has_above
        high_valid = (high > group) & has_below
        first = jnp.where(low_first, low, high)
        second = jnp.where(low_first, high, low)
        first_valid = (low_first & low_valid) | (jnp.logical_not(low_first) & high_valid)
        second_valid = (low_first & high_valid) | (jnp.logical_not(low_first) & low_valid)
        lag = chunks // 2
        for step in range(chunks + lag):
            if step < chunks:
                pass_sum(first_valid, first, step, first < group)
            if step >= lag:
                pass_sum(second_valid, second, step - lag, second < group)
        return carry

    lax.fori_loop(1, n_outer, sum_stage, 0)

    for chunk in range(chunks):
        columns = slice(chunk * width, (chunk + 1) * width)
        total = weighted(group, chunk) + hidden_ref[:, columns].astype(jnp.float32)
        sides = []
        for side, slot in ((has_above, group), (has_below, n_outer)):

            @pl.when(side)
            def _(slot=slot):
                arrived(sum_in.at[slot, chunk], sum_recv.at[slot * chunks + chunk])

            sides.append(
                jnp.where(side, sum_in[slot, chunk].astype(jnp.float32), 0.0)
            )
        out_ref[:, columns] = (total + sides[0] + sides[1]).astype(out_ref.dtype)

    for step in range(n_outer - 1):
        meta_copy(step).wait_send()
    for item in weight_copies():
        item.wait_send()

    def drain(block, carry):
        for chunk in range(chunks):

            @pl.when(has_above & (block <= group))
            def _():
                relay(block, chunk, True).wait_send()

            @pl.when(has_below & (block >= group))
            def _():
                relay(block, chunk, False).wait_send()

            for mate in mates:
                disp_copy(block, chunk, mate).wait_send()
                back_copy(block, chunk, mate).wait_send()

            @pl.when(block != group)
            def _():
                sum_copy(block, chunk, block < group).wait_send()

        return carry

    lax.fori_loop(0, n_outer, drain, 0)


EXPERT_LAG = 0
SUM_LAG = 1
TN = (((0,), (0,)), ((), ()))


def moe(tokens, meta, hidden, gate, up, down, n_sp, n_tp, cap):
    n_inner = math.gcd(n_sp, 4)
    n_outer = n_sp // n_inner
    rows, width = tokens.shape
    chunks = math.gcd(width // 128, 4)
    part = width // chunks
    slots = n_inner * cap
    dma = pltpu.SemaphoreType.DMA
    vmem = pltpu.VMEM
    blocks = n_outer * chunks
    low = jnp.bfloat16
    return pl.pallas_call(
        functools.partial(moe_kernel, n_outer, n_inner, n_tp, chunks),
        out_shape=jax.ShapeDtypeStruct((rows, width), low),
        in_specs=[VMEM] * 6,
        out_specs=VMEM,
        scratch_shapes=[
            vmem((n_outer, chunks, rows, part), low),
            vmem((n_outer,) + meta.shape, meta.dtype),
            vmem((n_outer, chunks, slots, part), low),
            vmem((n_outer, chunks, slots, part), low),
            vmem((n_outer, chunks, slots, part), low),
            vmem((n_outer, chunks, slots, part), low),
            vmem((n_outer, chunks, rows, part), low),
            vmem((n_outer + 1, chunks, rows, part), low),
            vmem((n_tp - 1,) + gate.shape, low),
            vmem((n_tp - 1,) + up.shape, low),
            vmem((n_tp - 1,) + down.shape, low),
            dma((n_outer - 1,)),
            dma((n_outer,)),
            dma((blocks,)),
            dma((blocks,)),
            dma((blocks,)),
            dma((blocks * n_inner,)),
            dma((blocks * n_inner,)),
            dma((blocks * n_inner,)),
            dma((blocks * n_inner,)),
            dma((blocks,)),
            dma((blocks + chunks,)),
            dma((3 * (n_tp - 1),)),
            dma((3 * (n_tp - 1),)),
        ],
        compiler_params=pltpu.CompilerParams(
            collective_id=1, has_side_effects=True, vmem_limit_bytes=67043328
        ),
        name="experts",
    )(tokens, meta, hidden, gate, up, down)


def local(
    residual,
    query_nope,
    query_rope,
    latent,
    key_rope,
    key_up,
    value_up,
    out_proj,
    norm_gain,
    routes,
    route_weight,
    w_gate,
    w_up,
    w_down,
):
    tp_count = lax.axis_size("tp")
    sp_count = lax.axis_size("sp")
    row_count = residual.shape[0]
    tok_dev = query_nope.shape[0]
    half = QK_ROPE // 2
    inverse = ROPE_BASE ** (-2.0 * jnp.arange(half, dtype=jnp.float32) / QK_ROPE)
    positions = lax.axis_index("sp") * tok_dev + jnp.arange(tok_dev, dtype=jnp.int32)
    angles = positions.astype(jnp.float32)[:, None] * jnp.tile(inverse, 4)[None, :]
    sign = jnp.tile(jnp.repeat(jnp.array([-1.0, 1.0], jnp.float32), half), 2)
    table = jnp.stack([jnp.cos(angles), jnp.sin(angles) * sign[None, :]])
    hidden, normed = attend(
        table,
        query_nope,
        query_rope,
        latent,
        key_rope,
        key_up,
        value_up,
        residual,
        norm_gain[None, :],
        out_proj,
        sp_count,
        tp_count,
    )
    expert_count = lax.axis_size("sp")
    capacity = max(2, 2 * (row_count * tp_count) // expert_count)
    capacity = -(-capacity // 16) * 16
    top_count = routes.shape[1]
    flat_expert = routes.reshape(-1)
    onehot = (flat_expert[:, None] == jnp.arange(expert_count, dtype=jnp.int32)[None, :]).astype(
        jnp.int32
    )
    slot_rank = jnp.sum(jnp.cumsum(onehot, axis=0) * onehot, axis=1) - 1
    slot_index = flat_expert * capacity + slot_rank
    slots = slot_index.reshape(row_count, top_count).astype(jnp.float32)
    meta = jnp.concatenate(
        [slots.T, route_weight.T, jnp.zeros((8 - 2 * top_count, row_count), jnp.float32)], axis=0
    )
    return moe(
        normed, meta, hidden, w_gate[0], w_up[0], w_down[0], sp_count, tp_count, capacity
    )


def solution(mesh):
    return jax.shard_map(
        local,
        mesh=mesh,
        in_specs=(
            P(("sp", "tp"), None),
            P("sp", "tp"),
            P("sp", "tp"),
            P(("sp", "tp"), None),
            P(("sp", "tp"), None),
            P(None, "tp"),
            P(None, "tp"),
            P(),
            P(),
            P(("sp", "tp"), None),
            P(("sp", "tp"), None),
            P("sp", None, "tp"),
            P("sp", None, "tp"),
            P("sp", "tp", None),
        ),
        out_specs=P(("sp", "tp"), None),
        check_vma=False,
    )
```

```python
import functools
import math

import jax
import jax.numpy as jnp
from jax import lax
from jax.experimental import pallas as pl
from jax.experimental.pallas import tpu as pltpu
from jax.sharding import PartitionSpec as P
import numpy as np

QK_NOPE = 128
QK_ROPE = 64
V_DIM = 128
SEGMENT = 64


EPSILON = 1e-06
ROPE_BASE = 10000.0
NEG_LARGE = -1e30


MESH = pl.DeviceIdType.MESH
VMEM = pl.BlockSpec(memory_space=pltpu.VMEM)


def greet(peers):
    barrier = pltpu.get_barrier_semaphore()
    for peer in peers:
        pl.semaphore_signal(barrier, inc=1, device_id=peer, device_id_type=MESH)
    pl.semaphore_wait(barrier, len(peers))


def arrived(block, semaphore):
    pltpu.make_async_copy(block, block, semaphore).wait()


def layer_kernel(
    n_outer,
    n_inner,
    n_tp,
    chunks,
    cap,
    inverse_hbm,
    routes_hbm,
    share_hbm,
    latent_hbm,
    key_rope_hbm,
    rope_hbm,
    nope_hbm,
    key_up_hbm,
    value_up_hbm,
    gain_hbm,
    residual_hbm,
    proj_hbm,
    gate_hbm,
    up_hbm,
    down_hbm,
    out_ref,
    inverse_ref,
    routes_ref,
    share_ref,
    latent_ref,
    key_rope_ref,
    rope_ref,
    nope_ref,
    key_up_ref,
    value_up_ref,
    gain_ref,
    residual_ref,
    proj_ref,
    gate_ref,
    up_ref,
    down_ref,
    table_ref,
    kv_ref,
    query_ref,
    value_ref,
    max_ref,
    sum_ref,
    acc_ref,
    own_ref,
    heads_ref,
    hidden_ref,
    tok_all,
    meta_ref,
    meta_all,
    disp_ref,
    in_ref,
    back_ref,
    sum_in,
    gate_all,
    up_all,
    down_all,
    load_sem,
    plane_send,
    mate_send,
    twin_send,
    kv_recv,
    heads_send,
    heads_recv,
    meta_send,
    meta_recv,
    above_send,
    below_send,
    tok_recv,
    disp_send,
    disp_recv,
    back_send,
    back_recv,
    sum_send,
    sum_recv,
    weight_send,
    weight_recv,
):
    sp, tp = lax.axis_index("sp"), lax.axis_index("tp")
    group, member = sp // n_inner, sp % n_inner
    queries = nope_ref.shape[0]
    rows, latent_width = latent_ref.shape
    heads = nope_ref.shape[1] // QK_NOPE
    packed = rows // (latent_width // QK_ROPE)
    scale = (QK_NOPE + QK_ROPE) ** (-0.5) * math.log2(math.e)
    width = residual_ref.shape[1] // chunks
    slots = n_inner * cap
    last = n_outer - 1
    has_above, has_below = group < last, group > 0
    cores = [(tp + hop) % n_tp for hop in range(1, n_tp)]
    places = [(member + step) % n_inner for step in range(n_inner)]
    mates = places[1:]
    twins = [(sp, core) for core in cores]

    loads = {}
    for number, (source, target) in enumerate(
        [
            (inverse_hbm, inverse_ref),
            (key_rope_hbm, key_rope_ref),
            (latent_hbm, latent_ref),
            (routes_hbm, routes_ref),
            (share_hbm, share_ref),
            (rope_hbm, rope_ref),
            (nope_hbm, nope_ref),
            (value_up_hbm, value_up_ref),
            (key_up_hbm, key_up_ref),
            (gain_hbm, gain_ref),
            (residual_hbm, residual_ref),
            (proj_hbm, proj_ref),
            (gate_hbm, gate_ref),
            (up_hbm, up_ref),
            (down_hbm, down_ref),
        ]
    ):
        loads[id(target)] = pltpu.make_async_copy(source, target, load_sem.at[number])
        loads[id(target)].start()

    def loaded(*refs):
        for ref in refs:
            loads[id(ref)].wait()

    def at(plane, place):
        return (plane * n_inner + place, tp)

    others = [at((group + step) % n_outer, member) for step in range(1, n_outer)]

    def copy(source, target, send_sem, recv_sem, peer):
        return pltpu.make_async_remote_copy(
            src_ref=source,
            dst_ref=target,
            send_sem=send_sem,
            recv_sem=recv_sem,
            device_id=peer,
            device_id_type=MESH,
        )

    def span(place):
        return pl.ds(pl.multiple_of(place * cap, cap), cap)

    def kv_copy(block, send_sem, peer):
        ref = kv_ref.at[block, tp]
        return copy(ref, ref, send_sem, kv_recv.at[block * n_tp + tp], peer)

    def plane_copy_kv(step):
        return kv_copy(sp, plane_send.at[step], at(group + step, member))

    def mate_copy(distance, step):
        return kv_copy(
            (group - distance) * n_inner + member,
            mate_send.at[distance * n_inner + step],
            at(group, places[step]),
        )

    def twin_copies(block):
        return [
            kv_copy(block, twin_send.at[block * (n_tp - 1) + hop], twin)
            for hop, twin in enumerate(twins)
        ]

    def landed(block, core):
        arrived(kv_ref.at[block, core], kv_recv.at[block * n_tp + core])

    def meta_copy(step):
        return copy(
            meta_ref, meta_all.at[group], meta_send.at[step], meta_recv.at[group], others[step]
        )

    def relay(block, chunk, upward):
        sems = above_send if upward else below_send
        ref = tok_all.at[block, chunk]
        number = block * chunks + chunk
        peer = at(group + 1 if upward else group - 1, member)
        return copy(ref, ref, sems.at[number], tok_recv.at[number], peer)

    def plane_copy(source, target, send_sem, recv_sem, block, chunk, mate):
        number = (block * chunks + chunk) * n_inner
        return copy(
            source.at[block, chunk, span(mate)],
            target.at[block, chunk, span(member)],
            send_sem.at[number + mate],
            recv_sem.at[number + member],
            at(group, mate),
        )

    def disp_copy(block, chunk, mate):
        return plane_copy(disp_ref, in_ref, disp_send, disp_recv, block, chunk, mate)

    def back_copy(block, chunk, mate):
        return plane_copy(disp_ref, back_ref, back_send, back_recv, block, chunk, mate)

    def plane_arrived(target, recv_sem, block, chunk):
        for mate in mates:
            arrived(
                target.at[block, chunk, span(mate)],
                recv_sem.at[(block * chunks + chunk) * n_inner + mate],
            )

    def sum_copy(block, chunk, downward):
        slot = jnp.where(downward | (block != group + 1), block, n_outer)
        peer = at(jnp.where(downward, group - 1, group + 1), member)
        return copy(
            tok_all.at[block, chunk],
            sum_in.at[slot, chunk],
            sum_send.at[block * chunks + chunk],
            sum_recv.at[slot * chunks + chunk],
            peer,
        )

    weights = [(gate_hbm, gate_all), (up_hbm, up_all), (down_hbm, down_all)]

    def weight_copies():
        for hop, twin in enumerate(twins):
            for number, (own, everyone) in enumerate(weights):
                slot = hop * 3 + number
                yield copy(
                    own, everyone.at[hop], weight_send.at[slot], weight_recv.at[slot], twin
                )

    first_slot = (group * slots).astype(jnp.float32)

    def named(block):
        numbers = first_slot + lax.broadcasted_iota(jnp.int32, (slots, rows), 0).astype(
            jnp.float32
        )
        meta = meta_all[block]
        return meta[0:1] == numbers, meta[1:2] == numbers, meta

    def scatter(block, chunk):
        one, two, unused = named(block)
        place = jnp.where(one | two, 1.0, 0.0).astype(jnp.bfloat16)
        disp_ref[block, chunk] = jnp.dot(
            place, tok_all[block, chunk], preferred_element_type=jnp.float32
        ).astype(jnp.bfloat16)
        for mate in mates:
            disp_copy(block, chunk, mate).start()
        in_ref[block, chunk, span(member)] = disp_ref[block, chunk, span(member)]

    def expert(block):
        for chunk in range(chunks):
            plane_arrived(in_ref, disp_recv, block, chunk)
        inputs = jnp.concatenate([in_ref[block, chunk] for chunk in range(chunks)], axis=1)
        halves = []
        for hop in range(n_tp):
            gate_half = gate_ref[...] if hop == 0 else gate_all[hop - 1]
            up_half = up_ref[...] if hop == 0 else up_all[hop - 1]
            gate = jnp.dot(inputs, gate_half, preferred_element_type=jnp.float32)
            up = jnp.dot(inputs, up_half, preferred_element_type=jnp.float32)
            halves.append((gate / (1.0 + jnp.exp(-gate)) * up).astype(jnp.bfloat16))
        for chunk in range(chunks):
            columns = slice(chunk * width, (chunk + 1) * width)
            made = jnp.dot(halves[0], down_ref[:, columns], preferred_element_type=jnp.float32)
            for hop in range(1, n_tp):
                made = made + jnp.dot(
                    halves[hop], down_all[hop - 1, :, columns], preferred_element_type=jnp.float32
                )
            for mate in mates:
                disp_copy(block, chunk, mate).wait_send()
            disp_ref[block, chunk] = made.astype(jnp.bfloat16)
            for mate in mates:
                back_copy(block, chunk, mate).start()
            back_ref[block, chunk, span(member)] = disp_ref[block, chunk, span(member)]

    def weighted(block, chunk):
        one, two, meta = named(block)
        shares = jnp.where(one, meta[2:3], 0.0) + jnp.where(two, meta[3:4], 0.0)
        high = shares.astype(jnp.bfloat16)
        low = (shares - high.astype(jnp.float32)).astype(jnp.bfloat16)
        plane_arrived(back_ref, back_recv, block, chunk)
        values = back_ref[block, chunk]
        return lax.dot_general(high, values, TN, preferred_element_type=jnp.float32) + (
            lax.dot_general(low, values, TN, preferred_element_type=jnp.float32)
        )

    def start_sum(block):
        downward = block < group

        @pl.when((downward & (group == last)) | ((block > group) & (group == 0)))
        def _():
            for chunk in range(chunks):
                tok_all[block, chunk] = weighted(block, chunk).astype(jnp.bfloat16)
                sum_copy(block, chunk, downward).start()

    def relay_sent(block, chunk):
        @pl.when(block < group)
        def _():
            relay(block, chunk, True).wait_send()

        @pl.when(block > group)
        def _():
            relay(block, chunk, False).wait_send()

    def pass_sum(valid, block, chunk, downward):
        @pl.when(valid)
        def _():
            total = weighted(block, chunk)
            relay_sent(block, chunk)
            arrived(sum_in.at[block, chunk], sum_recv.at[block * chunks + chunk])
            tok_all[block, chunk] = (
                total + sum_in[block, chunk].astype(jnp.float32)
            ).astype(jnp.bfloat16)
            sum_copy(block, chunk, downward).start()

    def both(distance, action):
        @pl.when(group >= distance)
        def _():
            action(group - distance)

        @pl.when((distance > 0) & (group + distance < n_outer))
        def _():
            action(group + distance)

    lane = lax.broadcasted_iota(jnp.int32, (1, 2 * QK_ROPE), 1)
    early = lane % QK_ROPE < QK_ROPE // 2

    def rotated(values, first):
        where = pl.ds(pl.multiple_of(first, values.shape[0]), values.shape[0])
        values = values.astype(jnp.float32)
        swapped = jnp.where(
            early,
            pltpu.roll(values, 2 * QK_ROPE - QK_ROPE // 2, 1),
            pltpu.roll(values, QK_ROPE // 2, 1),
        )
        return values * table_ref[0, where] + swapped * table_ref[1, where]

    loaded(inverse_ref)
    angles = (
        sp * queries + lax.broadcasted_iota(jnp.int32, (queries, 2 * QK_ROPE), 0)
    ).astype(jnp.float32) * inverse_ref[...]
    table_ref[0] = jnp.cos(angles)
    sines = jnp.sin(angles)
    table_ref[1] = jnp.where(early, -sines, sines)
    loaded(key_rope_ref)
    turned = key_rope_ref[...].astype(jnp.float32)
    wide_rope = jnp.concatenate([turned] * 2, axis=0).T
    loaded(latent_ref)
    key_rot = rotated(wide_rope, tp * rows)
    kv_ref[sp, tp, :rows] = latent_ref[...]
    for pair in range(latent_width // (2 * QK_ROPE)):
        low = key_rot[(2 * pair) * packed : (2 * pair + 1) * packed]
        high = key_rot[(2 * pair + 1) * packed : (2 * pair + 2) * packed]
        kv_ref[sp, tp, rows:, pair * 2 * QK_ROPE : (pair + 1) * 2 * QK_ROPE] = jnp.where(
            lane < QK_ROPE, low, high
        ).astype(jnp.bfloat16)

    loaded(routes_ref, share_ref)
    experts = lax.broadcasted_iota(jnp.int32, (n_inner * n_outer, rows), 0)
    chosen = [routes_ref[slot : slot + 1] == experts for slot in range(2)]
    named_here = jnp.where(chosen[0] | chosen[1], 1.0, 0.0).astype(jnp.bfloat16)
    earlier = jnp.where(
        lax.broadcasted_iota(jnp.int32, (rows, rows), 0)
        < lax.broadcasted_iota(jnp.int32, (rows, rows), 1),
        1.0,
        0.0,
    ).astype(jnp.bfloat16)
    ranks = jnp.dot(named_here, earlier, preferred_element_type=jnp.float32)
    for slot in range(2):
        number = jnp.where(chosen[slot], ranks + (experts * cap).astype(jnp.float32), 0.0)
        meta_ref[slot : slot + 1] = jnp.sum(number, axis=0, keepdims=True)
    meta_ref[2:4] = share_ref[...]
    meta_ref[4:8] = jnp.zeros((4, rows), jnp.float32)
    meta_all[group] = meta_ref[...]

    greet(others + [at(group, mate) for mate in mates] + twins)

    for item in twin_copies(sp):
        item.start()
    for step in range(1, max(n_inner, n_outer)):
        if step < n_outer:

            @pl.when(group + step < n_outer)
            def _():
                plane_copy_kv(step).start()

        if step < n_inner:

            @pl.when(places[step] > member)
            def _():
                mate_copy(0, step).start()

    for step in range(n_outer - 1):
        meta_copy(step).start()
    loaded(rope_ref, nope_ref, value_up_ref)
    for pair in range(0, heads, 2):
        turn = rotated(rope_ref[:, pair * QK_ROPE : (pair + 2) * QK_ROPE], 0).T
        for head in (pair, pair + 1):
            columns = slice(head * QK_NOPE, (head + 1) * QK_NOPE)
            query_ref[head, :QK_NOPE] = nope_ref[:, columns].astype(jnp.float32).T.astype(
                jnp.bfloat16
            )
            query_ref[head, QK_NOPE : QK_NOPE + QK_ROPE] = turn[
                (head - pair) * QK_ROPE : (head - pair + 1) * QK_ROPE
            ].astype(jnp.bfloat16)
            query_ref[head, QK_NOPE + QK_ROPE :] = jnp.zeros(
                (QK_ROPE, queries), jnp.bfloat16
            )
    value_ref[...] = value_up_ref[...].astype(jnp.float32).T.astype(jnp.bfloat16)

    def attend(blocks, own):
        latents, rots = [], []
        for block in blocks:
            for core in range(n_tp):
                latents.append(kv_ref[block, core, :rows])
                for pair in range(latent_width // (2 * QK_ROPE)):
                    part = kv_ref[
                        block, core, rows:, pair * 2 * QK_ROPE : (pair + 1) * 2 * QK_ROPE
                    ].astype(jnp.float32)
                    rots.append(part.astype(jnp.bfloat16))
                    rots.append(pltpu.roll(part, QK_ROPE, 1).astype(jnp.bfloat16))
        latent = jnp.concatenate(latents, axis=0)
        rot = jnp.concatenate(rots, axis=0)
        count = latent.shape[0]
        keys = jnp.dot(latent, key_up_ref[...], preferred_element_type=jnp.float32).astype(
            jnp.bfloat16
        )
        values = lax.dot_general(
            value_ref[...], latent, NT, preferred_element_type=jnp.float32
        ).astype(jnp.bfloat16)
        if own:
            allowed = (
                lax.broadcasted_iota(jnp.int32, (count, queries), 0) // SEGMENT
                <= lax.broadcasted_iota(jnp.int32, (count, queries), 1) // SEGMENT
            )
        for head in range(heads):
            wide = jnp.concatenate([keys[:, head * QK_NOPE : (head + 1) * QK_NOPE], rot], axis=1)
            scores = jnp.dot(wide, query_ref[head], preferred_element_type=jnp.float32)
            if own:
                scores = jnp.where(allowed, scores, NEG_LARGE)
            new_max = jnp.max(scores, axis=0, keepdims=True)
            if not own:
                old_max = max_ref[head]
                new_max = jnp.maximum(old_max, new_max)
                shrink = jnp.exp2((old_max - new_max) * scale)
            weights = jnp.exp2((scores - new_max) * scale)
            total = jnp.sum(weights, axis=0, keepdims=True)
            product = jnp.dot(
                values[head * V_DIM : (head + 1) * V_DIM],
                weights.astype(jnp.bfloat16),
                preferred_element_type=jnp.float32,
            )
            max_ref[head] = new_max
            if own:
                sum_ref[head] = total
                acc_ref[head] = product
            else:
                sum_ref[head] = sum_ref[head] * shrink + total
                acc_ref[head] = acc_ref[head] * shrink + product

    def from_plane(distance):
        block = (group - distance) * n_inner + member
        landed(block, tp)
        for step in range(1, n_inner):
            mate_copy(distance, step).start()
        for item in twin_copies(block):
            item.start()

    def from_mate(distance, step):
        block = (group - distance) * n_inner + places[step]
        landed(block, tp)
        for item in twin_copies(block):
            item.start()

    def ready(distance, step):
        block = (group - distance) * n_inner + places[step]
        for core in cores:
            landed(block, core)
        return block

    loaded(key_up_ref)
    attend([ready(0, 0)], True)

    @pl.when(group >= 1)
    def _():
        from_plane(1)

    for step in range(1, n_inner):

        @pl.when(places[step] < member)
        def _():
            from_mate(0, step)

    for item in weight_copies():
        item.start()

    @pl.when(group >= 2)
    def _():
        from_plane(2)

    def inside(step, carry):
        mate = (member + step) % n_inner

        @pl.when(mate < member)
        def _():
            block = group * n_inner + mate
            for core in cores:
                landed(block, core)
            attend([block], False)

        return carry

    lax.fori_loop(1, n_inner, inside, 0)

    unit = 2 if n_inner % 2 == 0 else 1

    def lead(distance, first):
        for step in range(first, first + unit):
            if step > 0:
                from_mate(distance, step)

    @pl.when(group >= 1)
    def _():
        lead(1, 0)

    def outside(distance, carry):
        @pl.when(distance + 2 <= group)
        def _():
            from_plane(distance + 2)

        for first in range(0, n_inner, unit):
            if first + unit < n_inner:
                lead(distance, first + unit)
            else:

                @pl.when(distance < group)
                def _():
                    lead(distance + 1, 0)

            attend([ready(distance, step) for step in range(first, first + unit)], False)
        return carry

    lax.fori_loop(1, group + 1, outside, 0)

    def heads_copy(hop):
        return copy(
            own_ref.at[pl.ds(pl.multiple_of(cores[hop] * rows, rows), rows)],
            heads_ref.at[hop],
            heads_send.at[hop],
            heads_recv.at[hop],
            twins[hop],
        )

    for head in range(heads):
        own_ref[:, head * V_DIM : (head + 1) * V_DIM] = (
            (acc_ref[head] / sum_ref[head]).T.astype(own_ref.dtype)
        )
    for hop in range(n_tp - 1):
        heads_copy(hop).start()
    loaded(proj_ref, residual_ref, gain_ref)
    depth = heads * V_DIM

    def proj(core, columns):
        return proj_ref[pl.ds(pl.multiple_of(core * depth, depth), depth), columns]

    mine = own_ref[pl.ds(pl.multiple_of(tp * rows, rows), rows)]
    spans = [slice(chunk * width, (chunk + 1) * width) for chunk in range(chunks)]
    sums = []
    for columns in spans:
        sums.append(
            residual_ref[:, columns].astype(jnp.float32)
            + jnp.dot(mine, proj(tp, columns), preferred_element_type=jnp.float32)
        )
    for hop in range(n_tp - 1):
        arrived(heads_ref.at[hop], heads_recv.at[hop])
        for number, columns in enumerate(spans):
            sums[number] = sums[number] + jnp.dot(
                heads_ref[hop],
                proj((tp + n_tp - hop - 1) % n_tp, columns),
                preferred_element_type=jnp.float32,
            )
    square = jnp.zeros((rows, 1), jnp.float32)
    for number, columns in enumerate(spans):
        hidden = sums[number].astype(jnp.bfloat16)
        hidden_ref[:, columns] = hidden
        hidden = hidden.astype(jnp.float32)
        square = square + jnp.sum(hidden * hidden, axis=1, keepdims=True)
    factor = lax.rsqrt(square / (width * chunks) + EPSILON)
    for chunk, columns in enumerate(spans):
        tok_all[group, chunk] = (
            hidden_ref[:, columns].astype(jnp.float32) * factor * gain_ref[:, columns]
        ).astype(jnp.bfloat16)

        @pl.when(has_above)
        def _():
            relay(group, chunk, True).start()

        @pl.when(has_below)
        def _():
            relay(group, chunk, False).start()

    for chunk in range(chunks):
        scatter(group, chunk)

    def receive(block, chunk, upward):
        number = block * chunks + chunk
        arrived(tok_all.at[block, chunk], tok_recv.at[number])
        if chunk == 0:
            arrived(meta_all.at[block], meta_recv.at[block])

        @pl.when(has_above if upward else has_below)
        def _():
            relay(block, chunk, upward).start()

        scatter(block, chunk)

    def stage(distance, carry):
        for chunk in range(chunks):

            @pl.when(group >= distance)
            def _():
                receive(group - distance, chunk, True)

            @pl.when(group + distance < n_outer)
            def _():
                receive(group + distance, chunk, False)

            if chunk == EXPERT_LAG % chunks:

                @pl.when(distance == 1)
                def _():
                    loaded(gate_ref, up_ref, down_ref)
                    for item in weight_copies():
                        item.wait_recv()

                both(distance - 1, expert)
            if chunk == SUM_LAG % chunks:
                both(distance - 1, start_sum)
        return carry

    lax.fori_loop(1, n_outer, stage, 0)
    both(last, expert)
    both(last, start_sum)

    def sum_stage(distance, carry):
        low_first = 2 * group >= n_outer
        low, high = last - distance, distance + 0
        low_valid = (low < group) & has_above
        high_valid = (high > group) & has_below
        first = jnp.where(low_first, low, high)
        second = jnp.where(low_first, high, low)
        first_valid = (low_first & low_valid) | (jnp.logical_not(low_first) & high_valid)
        second_valid = (low_first & high_valid) | (jnp.logical_not(low_first) & low_valid)
        lag = chunks // 2
        for step in range(chunks + lag):
            if step < chunks:
                pass_sum(first_valid, first, step, first < group)
            if step >= lag:
                pass_sum(second_valid, second, step - lag, second < group)
        return carry

    lax.fori_loop(1, n_outer, sum_stage, 0)

    for chunk in range(chunks):
        columns = slice(chunk * width, (chunk + 1) * width)
        total = weighted(group, chunk) + hidden_ref[:, columns].astype(jnp.float32)
        sides = []
        for side, slot in ((has_above, group), (has_below, n_outer)):

            @pl.when(side)
            def _(slot=slot):
                arrived(sum_in.at[slot, chunk], sum_recv.at[slot * chunks + chunk])

            sides.append(
                jnp.where(side, sum_in[slot, chunk].astype(jnp.float32), 0.0)
            )
        out_ref[:, columns] = (total + sides[0] + sides[1]).astype(out_ref.dtype)

    for hop in range(n_tp - 1):
        heads_copy(hop).wait_send()
    for item in twin_copies(sp):
        item.wait_send()
    for step in range(1, n_outer):

        @pl.when(group + step < n_outer)
        def _():
            plane_copy_kv(step).wait_send()

    for step in range(1, n_inner):

        @pl.when(places[step] > member)
        def _():
            mate_copy(0, step).wait_send()

        @pl.when(places[step] < member)
        def _():
            for item in twin_copies(group * n_inner + places[step]):
                item.wait_send()

    def drain_kv(distance, carry):
        for step in range(n_inner):
            if step > 0:
                mate_copy(distance, step).wait_send()
            for item in twin_copies((group - distance) * n_inner + places[step]):
                item.wait_send()
        return carry

    lax.fori_loop(1, group + 1, drain_kv, 0)
    for step in range(n_outer - 1):
        meta_copy(step).wait_send()
    for item in weight_copies():
        item.wait_send()
    for chunk in range(chunks):

        @pl.when(has_above)
        def _():
            relay(group, chunk, True).wait_send()

        @pl.when(has_below)
        def _():
            relay(group, chunk, False).wait_send()

    def drain(block, carry):
        for chunk in range(chunks):
            for mate in mates:
                back_copy(block, chunk, mate).wait_send()

            @pl.when(block != group)
            def _():
                sum_copy(block, chunk, block < group).wait_send()

        return carry

    lax.fori_loop(0, n_outer, drain, 0)


EXPERT_LAG = 0
SUM_LAG = 1
NT = (((1,), (1,)), ((), ()))
TN = (((0,), (0,)), ((), ()))


def layer(inputs, n_sp, n_tp):
    (inverse, routes, share, latent, key_rope, rope, nope) = inputs[:7]
    (key_up, value_up, gain, residual, proj, gate, up, down) = inputs[7:]
    n_inner = math.gcd(n_sp, 4)
    n_outer = n_sp // n_inner
    queries = nope.shape[0]
    heads = nope.shape[1] // QK_NOPE
    rows, latent_width = latent.shape
    packed = rows // (latent_width // QK_ROPE)
    capacity = max(2, 2 * (rows * n_tp) // n_sp)
    capacity = -(-capacity // 16) * 16
    chunks = math.gcd(residual.shape[1] // 128, 4)
    part = residual.shape[1] // chunks
    slots = n_inner * capacity
    blocks = n_outer * chunks
    dma = pltpu.SemaphoreType.DMA
    vmem = pltpu.VMEM
    low, wide = jnp.bfloat16, jnp.float32
    return pl.pallas_call(
        functools.partial(layer_kernel, n_outer, n_inner, n_tp, chunks, capacity),
        out_shape=jax.ShapeDtypeStruct(residual.shape, low),
        in_specs=[pl.BlockSpec(memory_space=pltpu.HBM)] * len(inputs),
        out_specs=VMEM,
        scratch_shapes=[vmem(item.shape, item.dtype) for item in inputs]
        + [
            vmem((2, queries, 2 * QK_ROPE), wide),
            vmem((n_sp, n_tp, rows + packed, latent_width), low),
            vmem((heads, QK_NOPE + 2 * QK_ROPE, queries), low),
            vmem((heads * V_DIM, latent_width), low),
            vmem((heads, 1, queries), wide),
            vmem((heads, 1, queries), wide),
            vmem((heads, V_DIM, queries), wide),
            vmem((queries, heads * V_DIM), low),
            vmem((n_tp - 1, rows, heads * V_DIM), low),
            vmem(residual.shape, low),
            vmem((n_outer, chunks, rows, part), low),
            vmem((8, rows), wide),
            vmem((n_outer, 8, rows), wide),
            vmem((n_outer, chunks, slots, part), low),
            vmem((n_outer, chunks, slots, part), low),
            vmem((n_outer, chunks, slots, part), low),
            vmem((n_outer + 1, chunks, rows, part), low),
            vmem((n_tp - 1,) + gate.shape, low),
            vmem((n_tp - 1,) + up.shape, low),
            vmem((n_tp - 1,) + down.shape, low),
            dma((len(inputs),)),
            dma((n_outer,)),
            dma((n_sp,)),
            dma((n_sp * (n_tp - 1),)),
            dma((n_sp * n_tp,)),
            dma((n_tp - 1,)),
            dma((n_tp - 1,)),
            dma((n_outer - 1,)),
            dma((n_outer,)),
            dma((blocks,)),
            dma((blocks,)),
            dma((blocks,)),
            dma((blocks * n_inner,)),
            dma((blocks * n_inner,)),
            dma((blocks * n_inner,)),
            dma((blocks * n_inner,)),
            dma((blocks,)),
            dma((blocks + chunks,)),
            dma((3 * (n_tp - 1),)),
            dma((3 * (n_tp - 1),)),
        ],
        compiler_params=pltpu.CompilerParams(
            collective_id=0, has_side_effects=True, vmem_limit_bytes=VMEM_LIMIT
        ),
        name="layer",
    )(*inputs)


VMEM_LIMIT = 60 * 2**20


def local(
    residual,
    query_nope,
    query_rope,
    latent,
    key_rope,
    key_up,
    value_up,
    out_proj,
    norm_gain,
    routes,
    route_weight,
    w_gate,
    w_up,
    w_down,
):
    half = QK_ROPE // 2
    inverse = np.tile(ROPE_BASE ** (-2.0 * np.arange(half) / QK_ROPE), 4).astype(np.float32)
    return layer(
        [
            jnp.asarray(inverse[None, :]),
            routes.T,
            route_weight.T,
            latent,
            key_rope.T,
            query_rope,
            query_nope,
            key_up,
            value_up,
            norm_gain[None, :],
            residual,
            out_proj,
            w_gate[0],
            w_up[0],
            w_down[0],
        ],
        lax.axis_size("sp"),
        lax.axis_size("tp"),
    )


def solution(mesh):
    return jax.shard_map(
        local,
        mesh=mesh,
        in_specs=(
            P(("sp", "tp"), None),
            P("sp", "tp"),
            P("sp", "tp"),
            P(("sp", "tp"), None),
            P(("sp", "tp"), None),
            P(None, "tp"),
            P(None, "tp"),
            P(),
            P(),
            P(("sp", "tp"), None),
            P(("sp", "tp"), None),
            P("sp", None, "tp"),
            P("sp", None, "tp"),
            P("sp", "tp", None),
        ),
        out_specs=P(("sp", "tp"), None),
        check_vma=False,
    )
```

```python
import functools
import math

import jax
import jax.numpy as jnp
from jax import lax
from jax.experimental import pallas as pl
from jax.experimental.pallas import tpu as pltpu
from jax.sharding import PartitionSpec as P
import numpy as np

QK_NOPE = 128
QK_ROPE = 64
V_DIM = 128
SEGMENT = 64


EPSILON = 1e-06
ROPE_BASE = 10000.0
NEG_LARGE = -1e30


MESH = pl.DeviceIdType.MESH
VMEM = pl.BlockSpec(memory_space=pltpu.VMEM)


def greet(peers):
    barrier = pltpu.get_barrier_semaphore()
    for peer in peers:
        pl.semaphore_signal(barrier, inc=1, device_id=peer, device_id_type=MESH)
    pl.semaphore_wait(barrier, len(peers))


def arrived(block, semaphore):
    pltpu.make_async_copy(block, block, semaphore).wait()


def layer_kernel(
    n_outer,
    n_inner,
    n_tp,
    chunks,
    cap,
    inverse_hbm,
    routes_hbm,
    share_hbm,
    latent_hbm,
    key_rope_hbm,
    rope_hbm,
    nope_hbm,
    key_up_hbm,
    value_up_hbm,
    gain_hbm,
    residual_hbm,
    proj_hbm,
    gate_hbm,
    up_hbm,
    down_hbm,
    out_ref,
    inverse_ref,
    routes_ref,
    share_ref,
    latent_ref,
    key_rope_ref,
    rope_ref,
    nope_ref,
    key_up_ref,
    value_up_ref,
    gain_ref,
    residual_ref,
    proj_ref,
    gate_ref,
    up_ref,
    down_ref,
    table_ref,
    kv_ref,
    query_ref,
    value_ref,
    max_ref,
    sum_ref,
    acc_ref,
    own_ref,
    heads_ref,
    hidden_ref,
    tok_all,
    meta_ref,
    meta_all,
    disp_ref,
    in_ref,
    back_ref,
    sum_in,
    gate_all,
    up_all,
    down_all,
    load_sem,
    plane_send,
    mate_send,
    twin_send,
    kv_recv,
    heads_send,
    heads_recv,
    meta_send,
    meta_recv,
    above_send,
    below_send,
    far_send,
    tok_recv,
    disp_send,
    disp_recv,
    back_send,
    back_recv,
    sum_send,
    sum_recv,
    weight_send,
    weight_recv,
):
    sp, tp = lax.axis_index("sp"), lax.axis_index("tp")
    group, member = sp // n_inner, sp % n_inner
    queries = nope_ref.shape[0]
    rows, latent_width = latent_ref.shape
    heads = nope_ref.shape[1] // QK_NOPE
    packed = rows // (latent_width // QK_ROPE)
    scale = (QK_NOPE + QK_ROPE) ** (-0.5) * math.log2(math.e)
    width = residual_ref.shape[1] // chunks
    slots = n_inner * cap
    last = n_outer - 1
    has_above, has_below = group < last, group > 0
    cores = [(tp + hop) % n_tp for hop in range(1, n_tp)]
    places = [(member + step) % n_inner for step in range(n_inner)]
    mates = places[1:]
    twins = [(sp, core) for core in cores]

    loads = {}
    for number, (source, target) in enumerate(
        [
            (inverse_hbm, inverse_ref),
            (key_rope_hbm, key_rope_ref),
            (latent_hbm, latent_ref),
            (routes_hbm, routes_ref),
            (share_hbm, share_ref),
            (rope_hbm, rope_ref),
            (nope_hbm, nope_ref),
            (value_up_hbm, value_up_ref),
            (key_up_hbm, key_up_ref),
            (gain_hbm, gain_ref),
            (residual_hbm, residual_ref),
            (proj_hbm, proj_ref),
            (gate_hbm, gate_ref),
            (up_hbm, up_ref),
            (down_hbm, down_ref),
        ]
    ):
        loads[id(target)] = pltpu.make_async_copy(source, target, load_sem.at[number])
        loads[id(target)].start()

    def loaded(*refs):
        for ref in refs:
            loads[id(ref)].wait()

    def at(plane, place):
        return (plane * n_inner + place, tp)

    others = [at((group + step) % n_outer, member) for step in range(1, n_outer)]

    def copy(source, target, send_sem, recv_sem, peer):
        return pltpu.make_async_remote_copy(
            src_ref=source,
            dst_ref=target,
            send_sem=send_sem,
            recv_sem=recv_sem,
            device_id=peer,
            device_id_type=MESH,
        )

    def span(place):
        return pl.ds(pl.multiple_of(place * cap, cap), cap)

    def kv_copy(block, send_sem, peer):
        ref = kv_ref.at[block, tp]
        return copy(ref, ref, send_sem, kv_recv.at[block * n_tp + tp], peer)

    def plane_copy_kv(step):
        return kv_copy(sp, plane_send.at[step], at(group + step, member))

    def mate_copy(distance, step):
        return kv_copy(
            (group - distance) * n_inner + member,
            mate_send.at[distance * n_inner + step],
            at(group, places[step]),
        )

    def twin_copies(block):
        return [
            kv_copy(block, twin_send.at[block * (n_tp - 1) + hop], twin)
            for hop, twin in enumerate(twins)
        ]

    def landed(block, core):
        arrived(kv_ref.at[block, core], kv_recv.at[block * n_tp + core])

    def meta_copy(step):
        return copy(
            meta_ref, meta_all.at[group], meta_send.at[step], meta_recv.at[group], others[step]
        )

    def relay(block, chunk, upward):
        sems = above_send if upward else below_send
        ref = tok_all.at[block, chunk]
        number = block * chunks + chunk
        peer = at(group + 1 if upward else group - 1, member)
        return copy(ref, ref, sems.at[number], tok_recv.at[number], peer)

    sends_far = (group == 0) & (n_outer > 2)

    def passes(block):
        return has_above & ((n_outer == 2) | (block != 0) | (group != last - 1))

    def far_copy(chunk):
        ref = tok_all.at[group, chunk]
        number = group * chunks + chunk
        return copy(ref, ref, far_send.at[chunk], tok_recv.at[number], at(last, member))

    def below(order):
        first_far = (group == last) & (n_outer > 2)
        return group - jnp.where(first_far, jnp.where(order == 1, last, order - 1), order)

    def plane_copy(source, target, send_sem, recv_sem, block, chunk, mate):
        number = (block * chunks + chunk) * n_inner
        return copy(
            source.at[block, chunk, span(mate)],
            target.at[block, chunk, span(member)],
            send_sem.at[number + mate],
            recv_sem.at[number + member],
            at(group, mate),
        )

    def disp_copy(block, chunk, mate):
        return plane_copy(disp_ref, in_ref, disp_send, disp_recv, block, chunk, mate)

    def back_copy(block, chunk, mate):
        return plane_copy(disp_ref, back_ref, back_send, back_recv, block, chunk, mate)

    def plane_arrived(target, recv_sem, block, chunk):
        for mate in mates:
            arrived(
                target.at[block, chunk, span(mate)],
                recv_sem.at[(block * chunks + chunk) * n_inner + mate],
            )

    def sum_copy(block, chunk, downward):
        slot = jnp.where(downward | (block != group + 1), block, n_outer)
        peer = at(jnp.where(downward, group - 1, group + 1), member)
        return copy(
            tok_all.at[block, chunk],
            sum_in.at[slot, chunk],
            sum_send.at[block * chunks + chunk],
            sum_recv.at[slot * chunks + chunk],
            peer,
        )

    weights = [(gate_hbm, gate_all), (up_hbm, up_all), (down_hbm, down_all)]

    def weight_copies():
        for hop, twin in enumerate(twins):
            for number, (own, everyone) in enumerate(weights):
                slot = hop * 3 + number
                yield copy(
                    own, everyone.at[hop], weight_send.at[slot], weight_recv.at[slot], twin
                )

    first_slot = (group * slots).astype(jnp.float32)

    def named(block):
        numbers = first_slot + lax.broadcasted_iota(jnp.int32, (slots, rows), 0).astype(
            jnp.float32
        )
        meta = meta_all[block]
        return meta[0:1] == numbers, meta[1:2] == numbers, meta

    def scatter(block, chunk):
        one, two, unused = named(block)
        place = jnp.where(one | two, 1.0, 0.0).astype(jnp.bfloat16)
        disp_ref[block, chunk] = jnp.dot(
            place, tok_all[block, chunk], preferred_element_type=jnp.float32
        ).astype(jnp.bfloat16)
        for mate in mates:
            disp_copy(block, chunk, mate).start()
        in_ref[block, chunk, span(member)] = disp_ref[block, chunk, span(member)]

    def expert(block):
        for chunk in range(chunks):
            plane_arrived(in_ref, disp_recv, block, chunk)
        inputs = jnp.concatenate([in_ref[block, chunk] for chunk in range(chunks)], axis=1)
        halves = []
        for hop in range(n_tp):
            gate_half = gate_ref[...] if hop == 0 else gate_all[hop - 1]
            up_half = up_ref[...] if hop == 0 else up_all[hop - 1]
            gate = jnp.dot(inputs, gate_half, preferred_element_type=jnp.float32)
            up = jnp.dot(inputs, up_half, preferred_element_type=jnp.float32)
            halves.append((gate / (1.0 + jnp.exp(-gate)) * up).astype(jnp.bfloat16))
        for chunk in range(chunks):
            columns = slice(chunk * width, (chunk + 1) * width)
            made = jnp.dot(halves[0], down_ref[:, columns], preferred_element_type=jnp.float32)
            for hop in range(1, n_tp):
                made = made + jnp.dot(
                    halves[hop], down_all[hop - 1, :, columns], preferred_element_type=jnp.float32
                )
            for mate in mates:
                disp_copy(block, chunk, mate).wait_send()
            disp_ref[block, chunk] = made.astype(jnp.bfloat16)
            for mate in mates:
                back_copy(block, chunk, mate).start()
            back_ref[block, chunk, span(member)] = disp_ref[block, chunk, span(member)]

    def weighted(block, chunk):
        one, two, meta = named(block)
        shares = jnp.where(one, meta[2:3], 0.0) + jnp.where(two, meta[3:4], 0.0)
        high = shares.astype(jnp.bfloat16)
        low = (shares - high.astype(jnp.float32)).astype(jnp.bfloat16)
        plane_arrived(back_ref, back_recv, block, chunk)
        values = back_ref[block, chunk]
        return lax.dot_general(high, values, TN, preferred_element_type=jnp.float32) + (
            lax.dot_general(low, values, TN, preferred_element_type=jnp.float32)
        )

    def start_sum(block):
        downward = block < group

        @pl.when((downward & (group == last)) | ((block > group) & (group == 0)))
        def _():
            for chunk in range(chunks):
                tok_all[block, chunk] = weighted(block, chunk).astype(jnp.bfloat16)
                sum_copy(block, chunk, downward).start()

    def relay_sent(block, chunk):
        @pl.when((block < group) & passes(block))
        def _():
            relay(block, chunk, True).wait_send()

        @pl.when(block > group)
        def _():
            relay(block, chunk, False).wait_send()

    def pass_sum(valid, block, chunk, downward):
        @pl.when(valid)
        def _():
            total = weighted(block, chunk)
            relay_sent(block, chunk)
            arrived(sum_in.at[block, chunk], sum_recv.at[block * chunks + chunk])
            tok_all[block, chunk] = (
                total + sum_in[block, chunk].astype(jnp.float32)
            ).astype(jnp.bfloat16)
            sum_copy(block, chunk, downward).start()

    def both(distance, action):
        @pl.when(group >= distance)
        def _():
            action(jnp.where(distance == 0, group, below(distance)))

        @pl.when((distance > 0) & (group + distance < n_outer))
        def _():
            action(group + distance)

    lane = lax.broadcasted_iota(jnp.int32, (1, 2 * QK_ROPE), 1)
    early = lane % QK_ROPE < QK_ROPE // 2

    def rotated(values, first):
        where = pl.ds(pl.multiple_of(first, values.shape[0]), values.shape[0])
        values = values.astype(jnp.float32)
        swapped = jnp.where(
            early,
            pltpu.roll(values, 2 * QK_ROPE - QK_ROPE // 2, 1),
            pltpu.roll(values, QK_ROPE // 2, 1),
        )
        return values * table_ref[0, where] + swapped * table_ref[1, where]

    loaded(inverse_ref)
    angles = (
        sp * queries + lax.broadcasted_iota(jnp.int32, (queries, 2 * QK_ROPE), 0)
    ).astype(jnp.float32) * inverse_ref[...]
    table_ref[0] = jnp.cos(angles)
    sines = jnp.sin(angles)
    table_ref[1] = jnp.where(early, -sines, sines)
    loaded(key_rope_ref)
    turned = key_rope_ref[...].astype(jnp.float32)
    wide_rope = jnp.concatenate([turned] * 2, axis=0).T
    loaded(latent_ref)
    key_rot = rotated(wide_rope, tp * rows)
    kv_ref[sp, tp, :rows] = latent_ref[...]
    for pair in range(latent_width // (2 * QK_ROPE)):
        low = key_rot[(2 * pair) * packed : (2 * pair + 1) * packed]
        high = key_rot[(2 * pair + 1) * packed : (2 * pair + 2) * packed]
        kv_ref[sp, tp, rows:, pair * 2 * QK_ROPE : (pair + 1) * 2 * QK_ROPE] = jnp.where(
            lane < QK_ROPE, low, high
        ).astype(jnp.bfloat16)

    loaded(routes_ref, share_ref)
    experts = lax.broadcasted_iota(jnp.int32, (n_inner * n_outer, rows), 0)
    chosen = [routes_ref[slot : slot + 1] == experts for slot in range(2)]
    named_here = jnp.where(chosen[0] | chosen[1], 1.0, 0.0).astype(jnp.bfloat16)
    earlier = jnp.where(
        lax.broadcasted_iota(jnp.int32, (rows, rows), 0)
        < lax.broadcasted_iota(jnp.int32, (rows, rows), 1),
        1.0,
        0.0,
    ).astype(jnp.bfloat16)
    ranks = jnp.dot(named_here, earlier, preferred_element_type=jnp.float32)
    for slot in range(2):
        number = jnp.where(chosen[slot], ranks + (experts * cap).astype(jnp.float32), 0.0)
        meta_ref[slot : slot + 1] = jnp.sum(number, axis=0, keepdims=True)
    meta_ref[2:4] = share_ref[...]
    meta_ref[4:8] = jnp.zeros((4, rows), jnp.float32)
    meta_all[group] = meta_ref[...]

    greet(others + [at(group, mate) for mate in mates] + twins)

    for item in twin_copies(sp):
        item.start()
    for step in range(1, max(n_inner, n_outer)):
        if step < n_outer:

            @pl.when(group + step < n_outer)
            def _():
                plane_copy_kv(step).start()

        if step < n_inner:

            @pl.when(places[step] > member)
            def _():
                mate_copy(0, step).start()

    for step in range(n_outer - 1):
        meta_copy(step).start()
    loaded(rope_ref, nope_ref, value_up_ref)
    for pair in range(0, heads, 2):
        turn = rotated(rope_ref[:, pair * QK_ROPE : (pair + 2) * QK_ROPE], 0).T
        for head in (pair, pair + 1):
            columns = slice(head * QK_NOPE, (head + 1) * QK_NOPE)
            query_ref[head, :QK_NOPE] = nope_ref[:, columns].astype(jnp.float32).T.astype(
                jnp.bfloat16
            )
            query_ref[head, QK_NOPE : QK_NOPE + QK_ROPE] = turn[
                (head - pair) * QK_ROPE : (head - pair + 1) * QK_ROPE
            ].astype(jnp.bfloat16)
            query_ref[head, QK_NOPE + QK_ROPE :] = jnp.zeros(
                (QK_ROPE, queries), jnp.bfloat16
            )
    value_ref[...] = value_up_ref[...].astype(jnp.float32).T.astype(jnp.bfloat16)

    def attend(blocks, own):
        latents, rots = [], []
        for block in blocks:
            for core in range(n_tp):
                latents.append(kv_ref[block, core, :rows])
                for pair in range(latent_width // (2 * QK_ROPE)):
                    part = kv_ref[
                        block, core, rows:, pair * 2 * QK_ROPE : (pair + 1) * 2 * QK_ROPE
                    ].astype(jnp.float32)
                    rots.append(part.astype(jnp.bfloat16))
                    rots.append(pltpu.roll(part, QK_ROPE, 1).astype(jnp.bfloat16))
        latent = jnp.concatenate(latents, axis=0)
        rot = jnp.concatenate(rots, axis=0)
        count = latent.shape[0]
        keys = jnp.dot(latent, key_up_ref[...], preferred_element_type=jnp.float32).astype(
            jnp.bfloat16
        )
        values = lax.dot_general(
            value_ref[...], latent, NT, preferred_element_type=jnp.float32
        ).astype(jnp.bfloat16)
        if own:
            allowed = (
                lax.broadcasted_iota(jnp.int32, (count, queries), 0) // SEGMENT
                <= lax.broadcasted_iota(jnp.int32, (count, queries), 1) // SEGMENT
            )
        for head in range(heads):
            wide = jnp.concatenate([keys[:, head * QK_NOPE : (head + 1) * QK_NOPE], rot], axis=1)
            scores = jnp.dot(wide, query_ref[head], preferred_element_type=jnp.float32)
            if own:
                scores = jnp.where(allowed, scores, NEG_LARGE)
            new_max = jnp.max(scores, axis=0, keepdims=True)
            if not own:
                old_max = max_ref[head]
                new_max = jnp.maximum(old_max, new_max)
                shrink = jnp.exp2((old_max - new_max) * scale)
            weights = jnp.exp2((scores - new_max) * scale)
            total = jnp.sum(weights, axis=0, keepdims=True)
            product = jnp.dot(
                values[head * V_DIM : (head + 1) * V_DIM],
                weights.astype(jnp.bfloat16),
                preferred_element_type=jnp.float32,
            )
            max_ref[head] = new_max
            if own:
                sum_ref[head] = total
                acc_ref[head] = product
            else:
                sum_ref[head] = sum_ref[head] * shrink + total
                acc_ref[head] = acc_ref[head] * shrink + product

    def from_plane(distance):
        block = (group - distance) * n_inner + member
        landed(block, tp)
        for step in range(1, n_inner):
            mate_copy(distance, step).start()
        for item in twin_copies(block):
            item.start()

    def from_mate(distance, step):
        block = (group - distance) * n_inner + places[step]
        landed(block, tp)
        for item in twin_copies(block):
            item.start()

    def ready(distance, step):
        block = (group - distance) * n_inner + places[step]
        for core in cores:
            landed(block, core)
        return block

    loaded(key_up_ref)
    attend([ready(0, 0)], True)

    @pl.when(group >= 1)
    def _():
        from_plane(1)

    for step in range(1, n_inner):

        @pl.when(places[step] < member)
        def _():
            from_mate(0, step)

    @pl.when(group >= 2)
    def _():
        from_plane(2)

    unit = 2 if n_inner % 2 == 0 else 1

    def lead(distance, first):
        for step in range(first, first + unit):
            if step > 0:
                from_mate(distance, step)

    def inside(step, carry):
        mate = (member + step) % n_inner

        @pl.when((step == n_inner - 1) & (group >= 1))
        def _():
            lead(1, 0)

        @pl.when(mate < member)
        def _():
            block = group * n_inner + mate
            for core in cores:
                landed(block, core)
            attend([block], False)

        return carry

    lax.fori_loop(1, n_inner, inside, 0)

    def outside(distance, carry):
        @pl.when(distance + 2 <= group)
        def _():
            from_plane(distance + 2)

        for first in range(0, n_inner, unit):
            if first + unit < n_inner:
                lead(distance, first + unit)
            else:

                @pl.when(distance < group)
                def _():
                    lead(distance + 1, 0)

            attend([ready(distance, step) for step in range(first, first + unit)], False)
        return carry

    lax.fori_loop(1, group + 1, outside, 0)

    def heads_copy(hop):
        return copy(
            own_ref.at[pl.ds(pl.multiple_of(cores[hop] * rows, rows), rows)],
            heads_ref.at[hop],
            heads_send.at[hop],
            heads_recv.at[hop],
            twins[hop],
        )

    for head in range(heads):
        own_ref[:, head * V_DIM : (head + 1) * V_DIM] = (
            (acc_ref[head] / sum_ref[head]).T.astype(own_ref.dtype)
        )
    for hop in range(n_tp - 1):
        heads_copy(hop).start()
    for item in weight_copies():
        item.start()
    loaded(proj_ref, residual_ref, gain_ref)
    depth = heads * V_DIM

    def proj(core, columns):
        return proj_ref[pl.ds(pl.multiple_of(core * depth, depth), depth), columns]

    mine = own_ref[pl.ds(pl.multiple_of(tp * rows, rows), rows)]
    spans = [slice(chunk * width, (chunk + 1) * width) for chunk in range(chunks)]
    sums = []
    for columns in spans:
        sums.append(
            residual_ref[:, columns].astype(jnp.float32)
            + jnp.dot(mine, proj(tp, columns), preferred_element_type=jnp.float32)
        )
    for hop in range(n_tp - 1):
        arrived(heads_ref.at[hop], heads_recv.at[hop])
        for number, columns in enumerate(spans):
            sums[number] = sums[number] + jnp.dot(
                heads_ref[hop],
                proj((tp + n_tp - hop - 1) % n_tp, columns),
                preferred_element_type=jnp.float32,
            )
    square = jnp.zeros((rows, 1), jnp.float32)
    for number, columns in enumerate(spans):
        hidden = sums[number].astype(jnp.bfloat16)
        hidden_ref[:, columns] = hidden
        hidden = hidden.astype(jnp.float32)
        square = square + jnp.sum(hidden * hidden, axis=1, keepdims=True)
    factor = lax.rsqrt(square / (width * chunks) + EPSILON)
    for chunk, columns in enumerate(spans):
        tok_all[group, chunk] = (
            hidden_ref[:, columns].astype(jnp.float32) * factor * gain_ref[:, columns]
        ).astype(jnp.bfloat16)

        @pl.when(has_above)
        def _():
            relay(group, chunk, True).start()

        @pl.when(has_below)
        def _():
            relay(group, chunk, False).start()

    @pl.when(sends_far)
    def _():
        for chunk in range(chunks):
            far_copy(chunk).start()

    for chunk in range(chunks):
        scatter(group, chunk)

    def receive(block, chunk, upward):
        number = block * chunks + chunk
        arrived(tok_all.at[block, chunk], tok_recv.at[number])
        if chunk == 0:
            arrived(meta_all.at[block], meta_recv.at[block])

        @pl.when(passes(block) if upward else has_below)
        def _():
            relay(block, chunk, upward).start()

        scatter(block, chunk)

    def stage(distance, carry):
        for chunk in range(chunks):

            @pl.when(group >= distance)
            def _():
                receive(below(distance), chunk, True)

            @pl.when(group + distance < n_outer)
            def _():
                receive(group + distance, chunk, False)

            if chunk in (EXPERT_EARLY, chunks - 1):

                @pl.when(((group > 0) & (group < last)) == (chunk == chunks - 1))
                def _():
                    @pl.when(distance == 1)
                    def _():
                        loaded(gate_ref, up_ref, down_ref)
                        for item in weight_copies():
                            item.wait_recv()

                    both(distance - 1, expert)

        @pl.when(distance > 1)
        def _():
            both(distance - 1, start_sum)

        return carry

    lax.fori_loop(1, n_outer, stage, 0)
    both(last, expert)
    both(last, start_sum)

    def sum_stage(distance, carry):
        low, high = distance - (last - group), distance + 1
        low_valid = (low >= 0) & (low < group) & has_above
        high_valid = (high > group) & has_below
        lag = SUM_GAP
        for step in range(chunks + lag):
            if step < chunks:
                pass_sum(high_valid, high, step, False)
            if step >= lag:
                pass_sum(low_valid, low, step - lag, True)
        return carry

    lax.fori_loop(1, last, sum_stage, 0)

    for chunk in range(chunks):
        columns = slice(chunk * width, (chunk + 1) * width)
        total = weighted(group, chunk) + hidden_ref[:, columns].astype(jnp.float32)
        sides = []
        for side, slot in ((has_above, group), (has_below, n_outer)):

            @pl.when(side)
            def _(slot=slot):
                arrived(sum_in.at[slot, chunk], sum_recv.at[slot * chunks + chunk])

            sides.append(
                jnp.where(side, sum_in[slot, chunk].astype(jnp.float32), 0.0)
            )
        out_ref[:, columns] = (total + sides[0] + sides[1]).astype(out_ref.dtype)

    for hop in range(n_tp - 1):
        heads_copy(hop).wait_send()
    for item in twin_copies(sp):
        item.wait_send()
    for step in range(1, n_outer):

        @pl.when(group + step < n_outer)
        def _():
            plane_copy_kv(step).wait_send()

    for step in range(1, n_inner):

        @pl.when(places[step] > member)
        def _():
            mate_copy(0, step).wait_send()

        @pl.when(places[step] < member)
        def _():
            for item in twin_copies(group * n_inner + places[step]):
                item.wait_send()

    def drain_kv(distance, carry):
        for step in range(n_inner):
            if step > 0:
                mate_copy(distance, step).wait_send()
            for item in twin_copies((group - distance) * n_inner + places[step]):
                item.wait_send()
        return carry

    lax.fori_loop(1, group + 1, drain_kv, 0)
    for step in range(n_outer - 1):
        meta_copy(step).wait_send()
    for item in weight_copies():
        item.wait_send()
    for chunk in range(chunks):

        @pl.when(sends_far)
        def _():
            far_copy(chunk).wait_send()

        @pl.when(has_above)
        def _():
            relay(group, chunk, True).wait_send()

        @pl.when(has_below)
        def _():
            relay(group, chunk, False).wait_send()

    def drain(block, carry):
        for chunk in range(chunks):
            for mate in mates:
                back_copy(block, chunk, mate).wait_send()

            @pl.when(block != group)
            def _():
                sum_copy(block, chunk, block < group).wait_send()

        return carry

    lax.fori_loop(0, n_outer, drain, 0)


SUM_GAP = 0
EXPERT_EARLY = 1
NT = (((1,), (1,)), ((), ()))
TN = (((0,), (0,)), ((), ()))


def layer(inputs, n_sp, n_tp):
    (inverse, routes, share, latent, key_rope, rope, nope) = inputs[:7]
    (key_up, value_up, gain, residual, proj, gate, up, down) = inputs[7:]
    n_inner = math.gcd(n_sp, 4)
    n_outer = n_sp // n_inner
    queries = nope.shape[0]
    heads = nope.shape[1] // QK_NOPE
    rows, latent_width = latent.shape
    packed = rows // (latent_width // QK_ROPE)
    capacity = max(2, 2 * (rows * n_tp) // n_sp)
    capacity = -(-capacity // 16) * 16
    chunks = math.gcd(residual.shape[1] // 128, 4)
    part = residual.shape[1] // chunks
    slots = n_inner * capacity
    blocks = n_outer * chunks
    dma = pltpu.SemaphoreType.DMA
    vmem = pltpu.VMEM
    low, wide = jnp.bfloat16, jnp.float32
    return pl.pallas_call(
        functools.partial(layer_kernel, n_outer, n_inner, n_tp, chunks, capacity),
        out_shape=jax.ShapeDtypeStruct(residual.shape, low),
        in_specs=[pl.BlockSpec(memory_space=pltpu.HBM)] * len(inputs),
        out_specs=VMEM,
        scratch_shapes=[vmem(item.shape, item.dtype) for item in inputs]
        + [
            vmem((2, queries, 2 * QK_ROPE), wide),
            vmem((n_sp, n_tp, rows + packed, latent_width), low),
            vmem((heads, QK_NOPE + 2 * QK_ROPE, queries), low),
            vmem((heads * V_DIM, latent_width), low),
            vmem((heads, 1, queries), wide),
            vmem((heads, 1, queries), wide),
            vmem((heads, V_DIM, queries), wide),
            vmem((queries, heads * V_DIM), low),
            vmem((n_tp - 1, rows, heads * V_DIM), low),
            vmem(residual.shape, low),
            vmem((n_outer, chunks, rows, part), low),
            vmem((8, rows), wide),
            vmem((n_outer, 8, rows), wide),
            vmem((n_outer, chunks, slots, part), low),
            vmem((n_outer, chunks, slots, part), low),
            vmem((n_outer, chunks, slots, part), low),
            vmem((n_outer + 1, chunks, rows, part), low),
            vmem((n_tp - 1,) + gate.shape, low),
            vmem((n_tp - 1,) + up.shape, low),
            vmem((n_tp - 1,) + down.shape, low),
            dma((len(inputs),)),
            dma((n_outer,)),
            dma((n_sp,)),
            dma((n_sp * (n_tp - 1),)),
            dma((n_sp * n_tp,)),
            dma((n_tp - 1,)),
            dma((n_tp - 1,)),
            dma((n_outer - 1,)),
            dma((n_outer,)),
            dma((blocks,)),
            dma((blocks,)),
            dma((chunks,)),
            dma((blocks,)),
            dma((blocks * n_inner,)),
            dma((blocks * n_inner,)),
            dma((blocks * n_inner,)),
            dma((blocks * n_inner,)),
            dma((blocks,)),
            dma((blocks + chunks,)),
            dma((3 * (n_tp - 1),)),
            dma((3 * (n_tp - 1),)),
        ],
        compiler_params=pltpu.CompilerParams(
            collective_id=0, has_side_effects=True, vmem_limit_bytes=VMEM_LIMIT
        ),
        name="layer",
    )(*inputs)


VMEM_LIMIT = 60 * 2**20


def local(
    residual,
    query_nope,
    query_rope,
    latent,
    key_rope,
    key_up,
    value_up,
    out_proj,
    norm_gain,
    routes,
    route_weight,
    w_gate,
    w_up,
    w_down,
):
    half = QK_ROPE // 2
    inverse = np.tile(ROPE_BASE ** (-2.0 * np.arange(half) / QK_ROPE), 4).astype(np.float32)
    return layer(
        [
            jnp.asarray(inverse[None, :]),
            routes.T,
            route_weight.T,
            latent,
            key_rope.T,
            query_rope,
            query_nope,
            key_up,
            value_up,
            norm_gain[None, :],
            residual,
            out_proj,
            w_gate[0],
            w_up[0],
            w_down[0],
        ],
        lax.axis_size("sp"),
        lax.axis_size("tp"),
    )


def solution(mesh):
    return jax.shard_map(
        local,
        mesh=mesh,
        in_specs=(
            P(("sp", "tp"), None),
            P("sp", "tp"),
            P("sp", "tp"),
            P(("sp", "tp"), None),
            P(("sp", "tp"), None),
            P(None, "tp"),
            P(None, "tp"),
            P(),
            P(),
            P(("sp", "tp"), None),
            P(("sp", "tp"), None),
            P("sp", None, "tp"),
            P("sp", None, "tp"),
            P("sp", "tp", None),
        ),
        out_specs=P(("sp", "tp"), None),
        check_vma=False,
    )
```

```python
import functools
import math

import jax
import jax.numpy as jnp
from jax import lax
from jax.experimental import pallas as pl
from jax.experimental.pallas import tpu as pltpu
from jax.sharding import PartitionSpec as P
import numpy as np

QK_NOPE = 128
QK_ROPE = 64
V_DIM = 128
SEGMENT = 64


EPSILON = 1e-06
ROPE_BASE = 10000.0
NEG_LARGE = -1e30


MESH = pl.DeviceIdType.MESH
VMEM = pl.BlockSpec(memory_space=pltpu.VMEM)


def greet(peers):
    barrier = pltpu.get_barrier_semaphore()
    for peer in peers:
        pl.semaphore_signal(barrier, inc=1, device_id=peer, device_id_type=MESH)
    pl.semaphore_wait(barrier, len(peers))


def arrived(block, semaphore):
    pltpu.make_async_copy(block, block, semaphore).wait()


def layer_kernel(
    n_outer,
    n_inner,
    n_tp,
    chunks,
    cap,
    inverse_hbm,
    routes_hbm,
    share_hbm,
    latent_hbm,
    key_rope_hbm,
    rope_hbm,
    nope_hbm,
    key_up_hbm,
    value_up_hbm,
    gain_hbm,
    residual_hbm,
    proj_hbm,
    gate_hbm,
    up_hbm,
    down_hbm,
    out_ref,
    inverse_ref,
    routes_ref,
    share_ref,
    latent_ref,
    key_rope_ref,
    rope_ref,
    nope_ref,
    key_up_ref,
    value_up_ref,
    gain_ref,
    residual_ref,
    proj_ref,
    gate_ref,
    up_ref,
    down_ref,
    table_ref,
    kv_ref,
    query_ref,
    value_ref,
    max_ref,
    sum_ref,
    acc_ref,
    own_ref,
    heads_ref,
    hidden_ref,
    tok_all,
    meta_ref,
    meta_all,
    disp_ref,
    in_ref,
    back_ref,
    sum_in,
    gate_all,
    up_all,
    down_all,
    load_sem,
    plane_send,
    mate_send,
    twin_send,
    kv_recv,
    heads_send,
    heads_recv,
    meta_send,
    meta_recv,
    above_send,
    below_send,
    far_send,
    tok_recv,
    disp_send,
    disp_recv,
    back_send,
    back_recv,
    sum_send,
    sum_recv,
    weight_send,
    weight_recv,
):
    sp, tp = lax.axis_index("sp"), lax.axis_index("tp")
    group, member = sp // n_inner, sp % n_inner
    queries = nope_ref.shape[0]
    rows, latent_width = latent_ref.shape
    heads = nope_ref.shape[1] // QK_NOPE
    packed = rows // (latent_width // QK_ROPE)
    scale = (QK_NOPE + QK_ROPE) ** (-0.5) * math.log2(math.e)
    width = residual_ref.shape[1] // chunks
    slots = n_inner * cap
    last = n_outer - 1
    has_above, has_below = group < last, group > 0
    cores = [(tp + hop) % n_tp for hop in range(1, n_tp)]
    places = [(member + step) % n_inner for step in range(n_inner)]
    mates = places[1:]
    twins = [(sp, core) for core in cores]

    loads = {}
    for number, (source, target) in enumerate(
        [
            (inverse_hbm, inverse_ref),
            (key_rope_hbm, key_rope_ref),
            (latent_hbm, latent_ref),
            (routes_hbm, routes_ref),
            (share_hbm, share_ref),
            (rope_hbm, rope_ref),
            (nope_hbm, nope_ref),
            (value_up_hbm, value_up_ref),
            (key_up_hbm, key_up_ref),
            (gain_hbm, gain_ref),
            (residual_hbm, residual_ref),
            (proj_hbm, proj_ref),
            (gate_hbm, gate_ref),
            (up_hbm, up_ref),
            (down_hbm, down_ref),
        ]
    ):
        loads[id(target)] = pltpu.make_async_copy(source, target, load_sem.at[number])
        loads[id(target)].start()

    def loaded(*refs):
        for ref in refs:
            loads[id(ref)].wait()

    def at(plane, place):
        return (plane * n_inner + place, tp)

    others = [at((group + step) % n_outer, member) for step in range(1, n_outer)]

    def copy(source, target, send_sem, recv_sem, peer):
        return pltpu.make_async_remote_copy(
            src_ref=source,
            dst_ref=target,
            send_sem=send_sem,
            recv_sem=recv_sem,
            device_id=peer,
            device_id_type=MESH,
        )

    def span(place):
        return pl.ds(pl.multiple_of(place * cap, cap), cap)

    def kv_copy(block, send_sem, peer):
        ref = kv_ref.at[block, tp]
        return copy(ref, ref, send_sem, kv_recv.at[block * n_tp + tp], peer)

    def plane_copy_kv(step):
        return kv_copy(sp, plane_send.at[step], at(group + step, member))

    def mate_copy(distance, step):
        return kv_copy(
            (group - distance) * n_inner + member,
            mate_send.at[distance * n_inner + step],
            at(group, places[step]),
        )

    def twin_copies(block):
        return [
            kv_copy(block, twin_send.at[block * (n_tp - 1) + hop], twin)
            for hop, twin in enumerate(twins)
        ]

    def landed(block, core):
        arrived(kv_ref.at[block, core], kv_recv.at[block * n_tp + core])

    def meta_copy(step):
        return copy(
            meta_ref, meta_all.at[group], meta_send.at[step], meta_recv.at[group], others[step]
        )

    def relay(block, chunk, upward):
        sems = above_send if upward else below_send
        ref = tok_all.at[block, chunk]
        number = block * chunks + chunk
        peer = at(group + 1 if upward else group - 1, member)
        return copy(ref, ref, sems.at[number], tok_recv.at[number], peer)

    sends_far = (group == 0) & (n_outer > 2)

    def passes(block):
        return has_above & ((n_outer == 2) | (block != 0) | (group != last - 1))

    def far_copy(chunk):
        ref = tok_all.at[group, chunk]
        number = group * chunks + chunk
        return copy(ref, ref, far_send.at[chunk], tok_recv.at[number], at(last, member))

    def below(order):
        first_far = (group == last) & (n_outer > 2)
        return group - jnp.where(first_far, jnp.where(order == 1, last, order - 1), order)

    def plane_copy(source, target, send_sem, recv_sem, block, chunk, mate):
        number = (block * chunks + chunk) * n_inner
        return copy(
            source.at[block, chunk, span(mate)],
            target.at[block, chunk, span(member)],
            send_sem.at[number + mate],
            recv_sem.at[number + member],
            at(group, mate),
        )

    def disp_copy(block, chunk, mate):
        return plane_copy(disp_ref, in_ref, disp_send, disp_recv, block, chunk, mate)

    def back_copy(block, chunk, mate):
        return plane_copy(disp_ref, back_ref, back_send, back_recv, block, chunk, mate)

    def plane_arrived(target, recv_sem, block, chunk):
        for mate in mates:
            arrived(
                target.at[block, chunk, span(mate)],
                recv_sem.at[(block * chunks + chunk) * n_inner + mate],
            )

    def sum_copy(block, chunk, downward):
        slot = jnp.where(downward | (block != group + 1), block, n_outer)
        peer = at(jnp.where(downward, group - 1, group + 1), member)
        return copy(
            tok_all.at[block, chunk],
            sum_in.at[slot, chunk],
            sum_send.at[block * chunks + chunk],
            sum_recv.at[slot * chunks + chunk],
            peer,
        )

    weights = [(gate_hbm, gate_all), (up_hbm, up_all), (down_hbm, down_all)]

    def weight_copies():
        for hop, twin in enumerate(twins):
            for number, (own, everyone) in enumerate(weights):
                slot = hop * 3 + number
                yield copy(
                    own, everyone.at[hop], weight_send.at[slot], weight_recv.at[slot], twin
                )

    first_slot = (group * slots).astype(jnp.float32)

    def named(block):
        numbers = first_slot + lax.broadcasted_iota(jnp.int32, (slots, rows), 0).astype(
            jnp.float32
        )
        meta = meta_all[block]
        return meta[0:1] == numbers, meta[1:2] == numbers, meta

    def scatter(block, chunk):
        one, two, unused = named(block)
        place = jnp.where(one | two, 1.0, 0.0).astype(jnp.bfloat16)
        disp_ref[block, chunk] = jnp.dot(
            place, tok_all[block, chunk], preferred_element_type=jnp.float32
        ).astype(jnp.bfloat16)
        for mate in mates:
            disp_copy(block, chunk, mate).start()
        in_ref[block, chunk, span(member)] = disp_ref[block, chunk, span(member)]

    def expert(block):
        for chunk in range(chunks):
            plane_arrived(in_ref, disp_recv, block, chunk)
        inputs = jnp.concatenate([in_ref[block, chunk] for chunk in range(chunks)], axis=1)
        halves = []
        for hop in range(n_tp):
            gate_half = gate_ref[...] if hop == 0 else gate_all[hop - 1]
            up_half = up_ref[...] if hop == 0 else up_all[hop - 1]
            gate = jnp.dot(inputs, gate_half, preferred_element_type=jnp.float32)
            up = jnp.dot(inputs, up_half, preferred_element_type=jnp.float32)
            halves.append((gate / (1.0 + jnp.exp(-gate)) * up).astype(jnp.bfloat16))
        for chunk in range(chunks):
            columns = slice(chunk * width, (chunk + 1) * width)
            made = jnp.dot(halves[0], down_ref[:, columns], preferred_element_type=jnp.float32)
            for hop in range(1, n_tp):
                made = made + jnp.dot(
                    halves[hop], down_all[hop - 1, :, columns], preferred_element_type=jnp.float32
                )
            for mate in mates:
                disp_copy(block, chunk, mate).wait_send()
            disp_ref[block, chunk] = made.astype(jnp.bfloat16)
            for mate in mates:
                back_copy(block, chunk, mate).start()
            back_ref[block, chunk, span(member)] = disp_ref[block, chunk, span(member)]

    def weighted(block, chunk):
        one, two, meta = named(block)
        shares = jnp.where(one, meta[2:3], 0.0) + jnp.where(two, meta[3:4], 0.0)
        high = shares.astype(jnp.bfloat16)
        low = (shares - high.astype(jnp.float32)).astype(jnp.bfloat16)
        plane_arrived(back_ref, back_recv, block, chunk)
        values = back_ref[block, chunk]
        return lax.dot_general(high, values, TN, preferred_element_type=jnp.float32) + (
            lax.dot_general(low, values, TN, preferred_element_type=jnp.float32)
        )

    def start_sum(block):
        downward = block < group

        @pl.when((downward & (group == last)) | ((block > group) & (group == 0)))
        def _():
            for chunk in range(chunks):
                tok_all[block, chunk] = weighted(block, chunk).astype(jnp.bfloat16)
                sum_copy(block, chunk, downward).start()

    def relay_sent(block, chunk):
        @pl.when((block < group) & passes(block))
        def _():
            relay(block, chunk, True).wait_send()

        @pl.when(block > group)
        def _():
            relay(block, chunk, False).wait_send()

    def pass_sum(valid, block, chunk, downward):
        @pl.when(valid)
        def _():
            total = weighted(block, chunk)
            relay_sent(block, chunk)
            arrived(sum_in.at[block, chunk], sum_recv.at[block * chunks + chunk])
            tok_all[block, chunk] = (
                total + sum_in[block, chunk].astype(jnp.float32)
            ).astype(jnp.bfloat16)
            sum_copy(block, chunk, downward).start()

    def both(distance, action):
        @pl.when(group >= distance)
        def _():
            action(jnp.where(distance == 0, group, below(distance)))

        @pl.when((distance > 0) & (group + distance < n_outer))
        def _():
            action(group + distance)

    lane = lax.broadcasted_iota(jnp.int32, (1, 2 * QK_ROPE), 1)
    early = lane % QK_ROPE < QK_ROPE // 2

    def rotated(values, first):
        where = pl.ds(pl.multiple_of(first, values.shape[0]), values.shape[0])
        values = values.astype(jnp.float32)
        swapped = jnp.where(
            early,
            pltpu.roll(values, 2 * QK_ROPE - QK_ROPE // 2, 1),
            pltpu.roll(values, QK_ROPE // 2, 1),
        )
        return values * table_ref[0, where] + swapped * table_ref[1, where]

    loaded(inverse_ref)
    angles = (
        sp * queries + lax.broadcasted_iota(jnp.int32, (queries, 2 * QK_ROPE), 0)
    ).astype(jnp.float32) * inverse_ref[...]
    table_ref[0] = jnp.cos(angles)
    sines = jnp.sin(angles)
    table_ref[1] = jnp.where(early, -sines, sines)
    loaded(key_rope_ref)
    turned = key_rope_ref[...].astype(jnp.float32)
    wide_rope = jnp.concatenate([turned] * 2, axis=0).T
    loaded(latent_ref)
    key_rot = rotated(wide_rope, tp * rows)
    kv_ref[sp, tp, :rows] = latent_ref[...]
    for pair in range(latent_width // (2 * QK_ROPE)):
        low = key_rot[(2 * pair) * packed : (2 * pair + 1) * packed]
        high = key_rot[(2 * pair + 1) * packed : (2 * pair + 2) * packed]
        kv_ref[sp, tp, rows:, pair * 2 * QK_ROPE : (pair + 1) * 2 * QK_ROPE] = jnp.where(
            lane < QK_ROPE, low, high
        ).astype(jnp.bfloat16)

    loaded(routes_ref, share_ref)
    experts = lax.broadcasted_iota(jnp.int32, (n_inner * n_outer, rows), 0)
    chosen = [routes_ref[slot : slot + 1] == experts for slot in range(2)]
    named_here = jnp.where(chosen[0] | chosen[1], 1.0, 0.0).astype(jnp.bfloat16)
    earlier = jnp.where(
        lax.broadcasted_iota(jnp.int32, (rows, rows), 0)
        < lax.broadcasted_iota(jnp.int32, (rows, rows), 1),
        1.0,
        0.0,
    ).astype(jnp.bfloat16)
    ranks = jnp.dot(named_here, earlier, preferred_element_type=jnp.float32)
    for slot in range(2):
        number = jnp.where(chosen[slot], ranks + (experts * cap).astype(jnp.float32), 0.0)
        meta_ref[slot : slot + 1] = jnp.sum(number, axis=0, keepdims=True)
    meta_ref[2:4] = share_ref[...]
    meta_ref[4:8] = jnp.zeros((4, rows), jnp.float32)
    meta_all[group] = meta_ref[...]

    greet(others + [at(group, mate) for mate in mates] + twins)

    for item in twin_copies(sp):
        item.start()
    for step in range(1, max(n_inner, n_outer)):
        if step < n_outer:

            @pl.when(group + step < n_outer)
            def _():
                plane_copy_kv(step).start()

        if step < n_inner:

            @pl.when(places[step] > member)
            def _():
                mate_copy(0, step).start()

    for step in range(n_outer - 1):
        meta_copy(step).start()
    loaded(rope_ref, nope_ref, value_up_ref)
    for pair in range(0, heads, 2):
        turn = rotated(rope_ref[:, pair * QK_ROPE : (pair + 2) * QK_ROPE], 0).T
        for head in (pair, pair + 1):
            columns = slice(head * QK_NOPE, (head + 1) * QK_NOPE)
            query_ref[head, :QK_NOPE] = nope_ref[:, columns].astype(jnp.float32).T.astype(
                jnp.bfloat16
            )
            query_ref[head, QK_NOPE : QK_NOPE + QK_ROPE] = turn[
                (head - pair) * QK_ROPE : (head - pair + 1) * QK_ROPE
            ].astype(jnp.bfloat16)
            query_ref[head, QK_NOPE + QK_ROPE :] = jnp.zeros(
                (QK_ROPE, queries), jnp.bfloat16
            )
    value_ref[...] = value_up_ref[...].astype(jnp.float32).T.astype(jnp.bfloat16)

    def attend(blocks, own):
        latents, rots = [], []
        for block in blocks:
            for core in range(n_tp):
                latents.append(kv_ref[block, core, :rows])
                for pair in range(latent_width // (2 * QK_ROPE)):
                    part = kv_ref[
                        block, core, rows:, pair * 2 * QK_ROPE : (pair + 1) * 2 * QK_ROPE
                    ].astype(jnp.float32)
                    rots.append(part.astype(jnp.bfloat16))
                    rots.append(pltpu.roll(part, QK_ROPE, 1).astype(jnp.bfloat16))
        latent = jnp.concatenate(latents, axis=0)
        rot = jnp.concatenate(rots, axis=0)
        count = latent.shape[0]
        keys = jnp.dot(latent, key_up_ref[...], preferred_element_type=jnp.float32).astype(
            jnp.bfloat16
        )
        values = lax.dot_general(
            value_ref[...], latent, NT, preferred_element_type=jnp.float32
        ).astype(jnp.bfloat16)
        if own:
            allowed = (
                lax.broadcasted_iota(jnp.int32, (count, queries), 0) // SEGMENT
                <= lax.broadcasted_iota(jnp.int32, (count, queries), 1) // SEGMENT
            )
        for head in range(heads):
            wide = jnp.concatenate([keys[:, head * QK_NOPE : (head + 1) * QK_NOPE], rot], axis=1)
            scores = jnp.dot(wide, query_ref[head], preferred_element_type=jnp.float32)
            if own:
                scores = jnp.where(allowed, scores, NEG_LARGE)
            new_max = jnp.max(scores, axis=0, keepdims=True)
            if not own:
                old_max = max_ref[head]
                new_max = jnp.maximum(old_max, new_max)
                shrink = jnp.exp2((old_max - new_max) * scale)
            weights = jnp.exp2((scores - new_max) * scale)
            total = jnp.sum(weights, axis=0, keepdims=True)
            product = jnp.dot(
                values[head * V_DIM : (head + 1) * V_DIM],
                weights.astype(jnp.bfloat16),
                preferred_element_type=jnp.float32,
            )
            max_ref[head] = new_max
            if own:
                sum_ref[head] = total
                acc_ref[head] = product
            else:
                sum_ref[head] = sum_ref[head] * shrink + total
                acc_ref[head] = acc_ref[head] * shrink + product

    def from_plane(distance):
        block = (group - distance) * n_inner + member
        landed(block, tp)
        for item in twin_copies(block):
            item.start()
        for step in range(n_inner - 1, 0, -1):
            mate_copy(distance, step).start()

    def from_mate(distance, step):
        block = (group - distance) * n_inner + places[step]
        landed(block, tp)
        for item in twin_copies(block):
            item.start()

    def ready(distance, step):
        block = (group - distance) * n_inner + places[step]
        for core in cores:
            landed(block, core)
        return block

    loaded(key_up_ref)
    attend([ready(0, 0)], True)

    @pl.when(group >= 1)
    def _():
        from_plane(1)

    for step in range(1, n_inner):

        @pl.when(places[step] < member)
        def _():
            from_mate(0, step)

    @pl.when(group >= 2)
    def _():
        from_plane(2)

    unit = 2 if n_inner % 2 == 0 else 1

    def lead(distance, first):
        for step in range(first, first + unit):
            if step > 0:
                from_mate(distance, step)

    def inside(step, carry):
        mate = (member + step) % n_inner

        @pl.when((step == n_inner - 1) & (group >= 1))
        def _():
            lead(1, 0)

        @pl.when(mate < member)
        def _():
            block = group * n_inner + mate
            for core in cores:
                landed(block, core)
            attend([block], False)

        return carry

    lax.fori_loop(1, n_inner, inside, 0)

    def outside(distance, carry):
        @pl.when(distance + 2 <= group)
        def _():
            from_plane(distance + 2)

        for first in range(0, n_inner, unit):
            if first + unit < n_inner:
                lead(distance, first + unit)
            else:

                @pl.when(distance < group)
                def _():
                    lead(distance + 1, 0)

            attend([ready(distance, step) for step in range(first, first + unit)], False)
        return carry

    lax.fori_loop(1, group + 1, outside, 0)

    def heads_copy(hop):
        return copy(
            own_ref.at[pl.ds(pl.multiple_of(cores[hop] * rows, rows), rows)],
            heads_ref.at[hop],
            heads_send.at[hop],
            heads_recv.at[hop],
            twins[hop],
        )

    for head in range(heads):
        own_ref[:, head * V_DIM : (head + 1) * V_DIM] = (
            (acc_ref[head] / sum_ref[head]).T.astype(own_ref.dtype)
        )
    for hop in range(n_tp - 1):
        heads_copy(hop).start()
    for item in weight_copies():
        item.start()
    loaded(proj_ref, residual_ref, gain_ref)
    depth = heads * V_DIM

    def proj(core, columns):
        return proj_ref[pl.ds(pl.multiple_of(core * depth, depth), depth), columns]

    mine = own_ref[pl.ds(pl.multiple_of(tp * rows, rows), rows)]
    spans = [slice(chunk * width, (chunk + 1) * width) for chunk in range(chunks)]
    sums = []
    for columns in spans:
        sums.append(
            residual_ref[:, columns].astype(jnp.float32)
            + jnp.dot(mine, proj(tp, columns), preferred_element_type=jnp.float32)
        )
    for hop in range(n_tp - 1):
        arrived(heads_ref.at[hop], heads_recv.at[hop])
        for number, columns in enumerate(spans):
            sums[number] = sums[number] + jnp.dot(
                heads_ref[hop],
                proj((tp + n_tp - hop - 1) % n_tp, columns),
                preferred_element_type=jnp.float32,
            )
    square = jnp.zeros((rows, 1), jnp.float32)
    for number, columns in enumerate(spans):
        hidden = sums[number].astype(jnp.bfloat16)
        hidden_ref[:, columns] = hidden
        hidden = hidden.astype(jnp.float32)
        square = square + jnp.sum(hidden * hidden, axis=1, keepdims=True)
    factor = lax.rsqrt(square / (width * chunks) + EPSILON)
    for chunk, columns in enumerate(spans):
        tok_all[group, chunk] = (
            hidden_ref[:, columns].astype(jnp.float32) * factor * gain_ref[:, columns]
        ).astype(jnp.bfloat16)

        @pl.when(has_above)
        def _():
            relay(group, chunk, True).start()

        @pl.when(has_below)
        def _():
            relay(group, chunk, False).start()

    @pl.when(sends_far)
    def _():
        for chunk in range(chunks):
            far_copy(chunk).start()

    for chunk in range(chunks):
        scatter(group, chunk)

    def receive(block, chunk, upward):
        number = block * chunks + chunk
        arrived(tok_all.at[block, chunk], tok_recv.at[number])
        if chunk == 0:
            arrived(meta_all.at[block], meta_recv.at[block])

        @pl.when(passes(block) if upward else has_below)
        def _():
            relay(block, chunk, upward).start()

        scatter(block, chunk)

    def stage(distance, carry):
        for chunk in range(chunks):

            @pl.when(group >= distance)
            def _():
                receive(below(distance), chunk, True)

            @pl.when(group + distance < n_outer)
            def _():
                receive(group + distance, chunk, False)

            if chunk in (EXPERT_EARLY, chunks - 1):

                @pl.when(((group > 0) & (group < last)) == (chunk == chunks - 1))
                def _():
                    @pl.when(distance == 1)
                    def _():
                        loaded(gate_ref, up_ref, down_ref)
                        for item in weight_copies():
                            item.wait_recv()

                    both(distance - 1, expert)

        @pl.when(distance > 1)
        def _():
            both(distance - 1, start_sum)

        return carry

    lax.fori_loop(1, n_outer, stage, 0)
    both(last, expert)
    both(last, start_sum)

    def sum_stage(distance, carry):
        low, high = distance - (last - group), distance + 1
        low_valid = (low >= 0) & (low < group) & has_above
        high_valid = (high > group) & has_below
        lag = SUM_GAP
        for step in range(chunks + lag):
            if step < chunks:
                pass_sum(high_valid, high, step, False)
            if step >= lag:
                pass_sum(low_valid, low, step - lag, True)
        return carry

    lax.fori_loop(1, last, sum_stage, 0)

    for chunk in range(chunks):
        columns = slice(chunk * width, (chunk + 1) * width)
        total = weighted(group, chunk) + hidden_ref[:, columns].astype(jnp.float32)
        sides = []
        for side, slot in ((has_above, group), (has_below, n_outer)):

            @pl.when(side)
            def _(slot=slot):
                arrived(sum_in.at[slot, chunk], sum_recv.at[slot * chunks + chunk])

            sides.append(
                jnp.where(side, sum_in[slot, chunk].astype(jnp.float32), 0.0)
            )
        out_ref[:, columns] = (total + sides[0] + sides[1]).astype(out_ref.dtype)

    for hop in range(n_tp - 1):
        heads_copy(hop).wait_send()
    for item in twin_copies(sp):
        item.wait_send()
    for step in range(1, n_outer):

        @pl.when(group + step < n_outer)
        def _():
            plane_copy_kv(step).wait_send()

    for step in range(1, n_inner):

        @pl.when(places[step] > member)
        def _():
            mate_copy(0, step).wait_send()

        @pl.when(places[step] < member)
        def _():
            for item in twin_copies(group * n_inner + places[step]):
                item.wait_send()

    def drain_kv(distance, carry):
        for step in range(n_inner):
            if step > 0:
                mate_copy(distance, step).wait_send()
            for item in twin_copies((group - distance) * n_inner + places[step]):
                item.wait_send()
        return carry

    lax.fori_loop(1, group + 1, drain_kv, 0)
    for step in range(n_outer - 1):
        meta_copy(step).wait_send()
    for item in weight_copies():
        item.wait_send()
    for chunk in range(chunks):

        @pl.when(sends_far)
        def _():
            far_copy(chunk).wait_send()

        @pl.when(has_above)
        def _():
            relay(group, chunk, True).wait_send()

        @pl.when(has_below)
        def _():
            relay(group, chunk, False).wait_send()

    def drain(block, carry):
        for chunk in range(chunks):
            for mate in mates:
                back_copy(block, chunk, mate).wait_send()

            @pl.when(block != group)
            def _():
                sum_copy(block, chunk, block < group).wait_send()

        return carry

    lax.fori_loop(0, n_outer, drain, 0)


SUM_GAP = 0
EXPERT_EARLY = 1
NT = (((1,), (1,)), ((), ()))
TN = (((0,), (0,)), ((), ()))


def layer(inputs, n_sp, n_tp):
    (inverse, routes, share, latent, key_rope, rope, nope) = inputs[:7]
    (key_up, value_up, gain, residual, proj, gate, up, down) = inputs[7:]
    n_inner = math.gcd(n_sp, 4)
    n_outer = n_sp // n_inner
    queries = nope.shape[0]
    heads = nope.shape[1] // QK_NOPE
    rows, latent_width = latent.shape
    packed = rows // (latent_width // QK_ROPE)
    capacity = max(2, 2 * (rows * n_tp) // n_sp)
    capacity = -(-capacity // 16) * 16
    chunks = math.gcd(residual.shape[1] // 128, 4)
    part = residual.shape[1] // chunks
    slots = n_inner * capacity
    blocks = n_outer * chunks
    dma = pltpu.SemaphoreType.DMA
    vmem = pltpu.VMEM
    low, wide = jnp.bfloat16, jnp.float32
    return pl.pallas_call(
        functools.partial(layer_kernel, n_outer, n_inner, n_tp, chunks, capacity),
        out_shape=jax.ShapeDtypeStruct(residual.shape, low),
        in_specs=[pl.BlockSpec(memory_space=pltpu.HBM)] * len(inputs),
        out_specs=VMEM,
        scratch_shapes=[vmem(item.shape, item.dtype) for item in inputs]
        + [
            vmem((2, queries, 2 * QK_ROPE), wide),
            vmem((n_sp, n_tp, rows + packed, latent_width), low),
            vmem((heads, QK_NOPE + 2 * QK_ROPE, queries), low),
            vmem((heads * V_DIM, latent_width), low),
            vmem((heads, 1, queries), wide),
            vmem((heads, 1, queries), wide),
            vmem((heads, V_DIM, queries), wide),
            vmem((queries, heads * V_DIM), low),
            vmem((n_tp - 1, rows, heads * V_DIM), low),
            vmem(residual.shape, low),
            vmem((n_outer, chunks, rows, part), low),
            vmem((8, rows), wide),
            vmem((n_outer, 8, rows), wide),
            vmem((n_outer, chunks, slots, part), low),
            vmem((n_outer, chunks, slots, part), low),
            vmem((n_outer, chunks, slots, part), low),
            vmem((n_outer + 1, chunks, rows, part), low),
            vmem((n_tp - 1,) + gate.shape, low),
            vmem((n_tp - 1,) + up.shape, low),
            vmem((n_tp - 1,) + down.shape, low),
            dma((len(inputs),)),
            dma((n_outer,)),
            dma((n_sp,)),
            dma((n_sp * (n_tp - 1),)),
            dma((n_sp * n_tp,)),
            dma((n_tp - 1,)),
            dma((n_tp - 1,)),
            dma((n_outer - 1,)),
            dma((n_outer,)),
            dma((blocks,)),
            dma((blocks,)),
            dma((chunks,)),
            dma((blocks,)),
            dma((blocks * n_inner,)),
            dma((blocks * n_inner,)),
            dma((blocks * n_inner,)),
            dma((blocks * n_inner,)),
            dma((blocks,)),
            dma((blocks + chunks,)),
            dma((3 * (n_tp - 1),)),
            dma((3 * (n_tp - 1),)),
        ],
        compiler_params=pltpu.CompilerParams(
            collective_id=0, has_side_effects=True, vmem_limit_bytes=VMEM_LIMIT
        ),
        name="layer",
    )(*inputs)


VMEM_LIMIT = 60 * 2**20


def local(
    residual,
    query_nope,
    query_rope,
    latent,
    key_rope,
    key_up,
    value_up,
    out_proj,
    norm_gain,
    routes,
    route_weight,
    w_gate,
    w_up,
    w_down,
):
    half = QK_ROPE // 2
    inverse = np.tile(ROPE_BASE ** (-2.0 * np.arange(half) / QK_ROPE), 4).astype(np.float32)
    return layer(
        [
            jnp.asarray(inverse[None, :]),
            routes.T,
            route_weight.T,
            latent,
            key_rope.T,
            query_rope,
            query_nope,
            key_up,
            value_up,
            norm_gain[None, :],
            residual,
            out_proj,
            w_gate[0],
            w_up[0],
            w_down[0],
        ],
        lax.axis_size("sp"),
        lax.axis_size("tp"),
    )


def solution(mesh):
    return jax.shard_map(
        local,
        mesh=mesh,
        in_specs=(
            P(("sp", "tp"), None),
            P("sp", "tp"),
            P("sp", "tp"),
            P(("sp", "tp"), None),
            P(("sp", "tp"), None),
            P(None, "tp"),
            P(None, "tp"),
            P(),
            P(),
            P(("sp", "tp"), None),
            P(("sp", "tp"), None),
            P("sp", None, "tp"),
            P("sp", None, "tp"),
            P("sp", "tp", None),
        ),
        out_specs=P(("sp", "tp"), None),
        check_vma=False,
    )
```
